32 devices in a mesh: sp: 8 (over z, x), tp: 4 (over y, core).
Axes of the slice: x: 2, y: 2, z: 4, core: 2. Of those that a mesh axis runs over, the one named last changes fastest.
Arguments:
- tokens: bfloat16 [1024, 2048], P('sp'), may hold values from -6 to 6
- norm_gain: float32 [2048], replicated, may hold values from 0.1 to 1.9
- cotangent: bfloat16 [1024, 2048], P('sp'), may hold values from -8 to 8
- routes: int32 [1024, 2], P('sp'), may hold values from 0 to 3, all different within a row; in each aligned block of 128 rows (0 to 127, 128 to 255, ...) at most 128 rows name the same one
- route_weight: float32 [1024, 2], P('sp'), may hold values from 0.2 to 1
- gate_weight: bfloat16 [8, 2048, 1792], P('sp', None, 'tp'), may hold values from -0.125 to 0.125
- up_weight: bfloat16 [8, 2048, 1792], P('sp', None, 'tp'), may hold values from -0.125 to 0.125
- down_weight: bfloat16 [8, 1792, 2048], P('sp', 'tp'), may hold values from -0.09375 to 0.09375
- scan_input: bfloat16 [1024, 1024], P('sp', 'tp'), may hold values from -6 to 6
- out_gate: bfloat16 [1024, 1024], P('sp', 'tp'), may hold values from -6 to 6
- step_size: float32 [16, 1024], P('tp', 'sp'), may hold values from 0.24 to 4.1
- decay_rate: float32 [16], P('tp'), may hold values from 9.667969e-06 to 0.031
- write_keys: bfloat16 [1024, 256], P('sp', 'tp'), may hold values from -0.75 to 0.75
- read_keys: bfloat16 [1024, 256], P('sp', 'tp'), may hold values from -0.75 to 0.75
- start_state: float32 [8, 16, 64, 64], P('sp', 'tp'), may hold values from -12 to 12
- out_proj: bfloat16 [2048, 1024], P(None, 'tp'), may hold values from -0.1875 to 0.1875
Outputs:
- residual_grad: bfloat16 [1024, 2048], P('sp', 'tp')
- gate_weight_grad: bfloat16 [8, 2048, 1792], P('sp', None, 'tp')
- up_weight_grad: bfloat16 [8, 2048, 1792], P('sp', None, 'tp')
- down_weight_grad: bfloat16 [8, 1792, 2048], P('sp', 'tp')
- out_proj_grad: float32 [2048, 1024], P('sp', 'tp')
- scan_input_grad: bfloat16 [1024, 1024], P('sp', 'tp')
- out_gate_grad: bfloat16 [1024, 1024], P('sp', 'tp')
- write_keys_grad: bfloat16 [1024, 256], P('sp', 'tp')
- read_keys_grad: bfloat16 [1024, 256], P('sp', 'tp')
The draws below stay inside these ranges and needn't reach their ends.
Inputs may be any that keep to these rules, and one draw needn't show every extreme that they name: Each token names two different experts. Among the tokens of one block of 128 positions at most 128 routes name one expert, and in every draw some expert gets exactly 128 routes from some block.
All inputs are finite; a program needn't handle non-finite values.
Results may differ from the reference program's by a relative error of at most 0.0078.
Values may be sent and summed in bfloat16 or wider, within the bound.
A program may use at most 128 MiB of HBM per device.

```python
import math
import jax
import jax.numpy as jnp
import numpy as np
from jax import lax

D = 2048
FF = 3584
FF_HALF = 1792
HEADS = 16
HEAD_DIM = 64
STATE = 64
GROUPS = 4
MIX = 1024
TOK_DEV = 128
BLOCKS = 8
TOKENS = 1024
EXPERTS = 4
CAP = 128
N_SP = 8


def draw_step_size(key, part):
    token_key, block_key = jax.random.split(jax.random.fold_in(key, 11))
    block_count = TOKENS // TOK_DEV
    local = jax.random.uniform(token_key, (HEADS, TOKENS), jnp.float32, -0.7, 0.7)
    slow = jax.random.uniform(block_key, (HEADS, block_count, 1), jnp.float32, -0.7, 0.7)
    slow = jnp.broadcast_to(slow, (HEADS, block_count, TOK_DEV)).reshape(HEADS, TOKENS)
    return jnp.exp(local + slow)


def draw_decay_rate(key, part):
    lowest = math.log(0.01 / TOKENS)
    highest = math.log(0.03)
    drawn = jax.random.uniform(jax.random.fold_in(key, 23), (HEADS,), jnp.float32, lowest, highest)
    return jnp.exp(drawn)


def spiked(array, key, source, target, shards_of, factor):
    owner, partner = [(jnp.arange(array.shape[dim]) // (array.shape[dim] // shards_of)).reshape([-1 if axis == dim else 1 for axis in range(array.ndim)]) for dim in (source, target)]
    chosen = jax.random.permutation(key, shards_of)[partner]
    strong = (owner == chosen) | (owner == (partner + shards_of // 2) % shards_of)
    return jnp.where(strong, factor * array, array)


def block_scale(own_key, shape, cuts, smallest, top_value):
    factor_of, own = 1.0, jax.random.fold_in(own_key, 6)
    for axis_at, blocks in cuts:
        heights = jnp.exp(jax.random.uniform(jax.random.fold_in(own, axis_at), (blocks,), jnp.float32, smallest / len(cuts), top_value / len(cuts)))
        factor_of = factor_of * jnp.repeat(heights, shape[axis_at] // blocks).reshape([-1 if axis == axis_at else 1 for axis in range(len(shape))])
    return factor_of


def deal_out(key, own, number, rows, number_of, top, reach, slope):
    order = jax.random.permutation(key, number_of)
    heavy_load, usual = load_shares(number_of, rows * top, reach, slope, True), load_shares(number_of, rows * top, reach, slope, False)
    places = jnp.arange(number_of)

    def named(sizes, turn):
        used = int((sizes > 0).sum())
        fixed = max(1, used // 4)
        shifted = fixed + (places - fixed + turn * (used - fixed)) % max(1, number_of - fixed)
        return jnp.zeros((number_of,), jnp.int32).at[order[jnp.where(places < fixed, places, shifted)]].set(jnp.asarray(sizes, jnp.int32))

    sizes = jnp.where(number % 4 == 0, named(heavy_load, number // 4), named(usual, number - number // 4 - 1))
    mixed = jax.random.permutation(jax.random.fold_in(own, 3), number_of)
    donor, sink = mixed[0:number_of // 2 * 2:2], mixed[1:number_of // 2 * 2:2]
    margin = jnp.minimum(sizes[donor] - 1, reach - sizes[sink]) // 2
    margin = jnp.where((donor == order[0]) | (sink == order[0]) | (sizes[sink] == 0), 0, jnp.maximum(margin, 0))
    shifted = jax.random.randint(jax.random.fold_in(own, 4), (number_of // 2,), 0, 1 << 20) % (margin + 1)
    sizes = sizes.at[donor].add(-shifted).at[sink].add(shifted)
    members = jnp.searchsorted(jnp.cumsum(sizes), jnp.arange(rows * top), side="right").astype(jnp.int32)
    listing = members.reshape(top, rows).T
    listing = listing[jax.random.permutation(jax.random.fold_in(own, 1), rows)]
    turn = jax.random.randint(jax.random.fold_in(own, 2), (rows, 1), 0, top)
    return jnp.take_along_axis(listing, (jnp.arange(top)[None, :] + turn) % top, axis=1)


def load_shares(count, total, reach, slope, full):
    loads = [(1 << 20) // math.isqrt(rank ** slope) + 1 for rank in range(1, count + 1)]
    largest = reach if full else min(reach, max(-(-total // count), total * loads[0] // sum(loads)))
    least = 1 if total - largest >= count - 1 else 0
    counts, surplus = [largest] + [least] * (count - 1), total - largest - least * (count - 1)
    while surplus > 0:
        free = [i for i in range(1, count) if counts[i] < largest] or [i for i in range(1, count) if counts[i] < reach]
        whole, budget = sum([loads[i] for i in free]), surplus
        for i in free:
            more = min(reach - counts[i], max(1, budget * loads[i] // whole), surplus)
            counts[i] = counts[i] + more
            surplus = surplus - more
    return np.array(counts)


def centred(stream_key, extent, scale, bound, cuts=(), kind=jnp.bfloat16):
    result = scale * jax.random.normal(stream_key, extent, jnp.float32)
    if cuts:
        result = result * block_scale(stream_key, extent, cuts, -0.22, 0.18)
    return jnp.clip(result, -bound, bound).astype(kind)


def noise_with(stream_key, shape, scale, reach, shards, heavy, dtype=jnp.bfloat16):
    values = scale * jax.random.normal(stream_key, shape, jnp.float32)
    if shards:
        values = values * block_scale(stream_key, shape, shards, -0.22, 0.18)
    return jnp.clip(spiked(values, jax.random.fold_in(stream_key, 3), *heavy), -reach, reach).astype(dtype)


def setup_inputs(seed: int = 0) -> dict:
    streams_of = jax.random.split(jax.random.key(seed), 17)
    tokens = centred(streams_of[0], (TOKENS, D), 1.0, 6.0, ((0, 8),))
    norm_gain = jnp.clip(1.0 + 0.18 * jax.random.normal(streams_of[1], (D,), jnp.float32), 0.1, 1.9)
    cotangent = noise_with(streams_of[2], (TOKENS, D), 1.0, 8.0, ((0, 8),), (0, 1, 8, 2.0))
    routes_keys = jax.random.split(jax.random.fold_in(streams_of[3], 1), TOKENS // TOK_DEV)
    routes_turns = jax.random.permutation(jax.random.fold_in(streams_of[3], 3), TOKENS // TOK_DEV)
    routes = jax.vmap(lambda own, number: deal_out(jax.random.fold_in(streams_of[3], 2), own, number, TOK_DEV, EXPERTS, 2, CAP, 1))(routes_keys, routes_turns).reshape((TOKENS, 2))
    route_weight = jnp.clip(0.2 + 0.8 * jax.random.uniform(streams_of[4], (TOKENS, 2), jnp.float32) ** block_scale(streams_of[4], (TOKENS, 2), ((0, 8),), -0.2, 0.2), 0.2, 1.0)
    gate_weight = centred(streams_of[5], (N_SP, D, FF_HALF), D ** -0.5, 0.125, ((0, 8), (2, 4)))
    up_weight = centred(streams_of[6], (N_SP, D, FF_HALF), D ** -0.5, 0.125, ((0, 8), (2, 4)))
    down_weight = centred(streams_of[7], (N_SP, FF_HALF, D), FF ** -0.5, 0.09375, ((0, 8), (1, 4)))
    scan_input = centred(streams_of[8], (TOKENS, MIX), 1.0, 6.0, ((0, 8), (1, 4)))
    out_gate = centred(streams_of[9], (TOKENS, MIX), 1.0, 6.0, ((0, 8), (1, 4)))
    step_size = draw_step_size(jax.random.fold_in(streams_of[16], 71), 0)
    decay_rate = draw_decay_rate(jax.random.fold_in(streams_of[16], 71), 0)
    write_keys = centred(streams_of[12], (TOKENS, GROUPS * STATE), 0.125, 0.75, ((0, 8), (1, 4)))
    read_keys = centred(streams_of[13], (TOKENS, GROUPS * STATE), 0.125, 0.75, ((0, 8), (1, 4)))
    start_state = centred(streams_of[14], (BLOCKS, HEADS, HEAD_DIM, STATE), 2.0, 12.0, ((0, 8), (1, 4)), jnp.float32)
    out_proj = centred(streams_of[15], (D, MIX), MIX ** -0.5, 0.1875, ((1, 4),))
    return dict(tokens=tokens, norm_gain=norm_gain, cotangent=cotangent, routes=routes, route_weight=route_weight, gate_weight=gate_weight, up_weight=up_weight, down_weight=down_weight, scan_input=scan_input, out_gate=out_gate, step_size=step_size, decay_rate=decay_rate, write_keys=write_keys, read_keys=read_keys, start_state=start_state, out_proj=out_proj)


EPS = 1e-06
HIGHEST = lax.Precision.HIGHEST

def prepare(scan_rows, step_rows, write_rows, read_rows, decay_rates, per_group):
    length = scan_rows.shape[0]
    head_count = step_rows.shape[0]
    logdec = jnp.cumsum(-decay_rates[:, None] * step_rows, axis=1)
    causal = jnp.arange(length)[:, None] >= jnp.arange(length)[None, :]
    spread = jnp.where(causal[None, :, :], logdec[:, :, None] - logdec[:, None, :], -jnp.inf)
    weights = jnp.exp(spread)
    inputs = scan_rows.astype(jnp.float32).reshape(length, head_count, -1) * jnp.transpose(step_rows)[:, :, None]
    write_head = jnp.repeat(write_rows.astype(jnp.float32).reshape(length, -1, STATE), per_group, axis=1)
    read_head = jnp.repeat(read_rows.astype(jnp.float32).reshape(length, -1, STATE), per_group, axis=1)
    scores = jnp.einsum('thn,shn->hts', read_head, write_head, precision=HIGHEST) * weights
    return (logdec, weights, inputs, write_head, read_head, scores)

def block_forward(scan_rows, gate_rows, step_rows, write_rows, read_rows, decay_rates, entry_state, mix_grad, per_group):
    logdec, weights, inputs, write_head, read_head, scores = prepare(scan_rows, step_rows, write_rows, read_rows, decay_rates, per_group)
    length, head_count = (inputs.shape[0], inputs.shape[1])
    growth = jnp.transpose(jnp.exp(logdec))
    output = jnp.einsum('hts,shp->thp', scores, inputs, precision=HIGHEST)
    output = output + growth[:, :, None] * jnp.einsum('thn,hpn->thp', read_head, entry_state, precision=HIGHEST)
    gate_val = gate_rows.astype(jnp.float32).reshape(length, head_count, -1)
    sigmoid_val = jax.nn.sigmoid(gate_val)
    gated = (output * gate_val * sigmoid_val).reshape(length, -1).astype(jnp.bfloat16)
    out_grad = mix_grad.reshape(length, head_count, -1)
    state_grad = out_grad * gate_val * sigmoid_val
    gate_grad = (out_grad * output * sigmoid_val * (1.0 + gate_val * (1.0 - sigmoid_val))).reshape(length, -1).astype(jnp.bfloat16)
    carried = jnp.einsum('th,thp,thn->hpn', growth, state_grad, read_head, precision=HIGHEST)
    return (gated, gate_grad, jnp.exp(logdec[:, -1]), carried, state_grad)

def block_back(scan_rows, step_rows, write_rows, read_rows, decay_rates, entry_state, state_grad, later_state, per_group):
    logdec, weights, inputs, write_head, read_head, scores = prepare(scan_rows, step_rows, write_rows, read_rows, decay_rates, per_group)
    length, head_count = (inputs.shape[0], inputs.shape[1])
    growth = jnp.transpose(jnp.exp(logdec))
    shrink = jnp.transpose(jnp.exp(logdec[:, -1:] - logdec))
    in_grad = jnp.einsum('hts,thp->shp', scores, state_grad, precision=HIGHEST)
    in_grad = in_grad + shrink[:, :, None] * jnp.einsum('shn,hpn->shp', write_head, later_state, precision=HIGHEST)
    scan_grad = (in_grad * jnp.transpose(step_rows)[:, :, None]).reshape(length, -1).astype(jnp.bfloat16)
    pair_terms = jnp.einsum('thp,shp->hts', state_grad, inputs, precision=HIGHEST) * weights
    read_grad = jnp.einsum('hts,shn->thn', pair_terms, write_head, precision=HIGHEST)
    read_grad = read_grad + growth[:, :, None] * jnp.einsum('thp,hpn->thn', state_grad, entry_state, precision=HIGHEST)
    write_grad = jnp.einsum('hts,thn->shn', pair_terms, read_head, precision=HIGHEST)
    write_grad = write_grad + shrink[:, :, None] * jnp.einsum('shp,hpn->shn', inputs, later_state, precision=HIGHEST)
    group_count = head_count // per_group
    read_total = lax.optimization_barrier(jnp.sum(read_grad.reshape(length, group_count, per_group, -1), axis=2)).reshape(length, -1).astype(jnp.bfloat16)
    write_total = lax.optimization_barrier(jnp.sum(write_grad.reshape(length, group_count, per_group, -1), axis=2)).reshape(length, -1).astype(jnp.bfloat16)
    return (scan_grad, write_total, read_total)

def expert_grads(rows_in, rows_cot, gate_mat, up_mat, down_mat):
    contract_rows = (((0,), (0,)), ((), ()))
    contract_cols = (((1,), (1,)), ((), ()))
    gate_pre = jnp.dot(rows_in, gate_mat, preferred_element_type=jnp.float32)
    up_pre = jnp.dot(rows_in, up_mat, preferred_element_type=jnp.float32)
    sigmoid_val = jax.nn.sigmoid(gate_pre)
    active = (gate_pre * sigmoid_val * up_pre).astype(jnp.bfloat16)
    down_grad = lax.dot_general(active, rows_cot, contract_rows, preferred_element_type=jnp.float32)
    act_grad = lax.dot_general(rows_cot, down_mat, contract_cols, preferred_element_type=jnp.float32)
    gate_pre_grad = (act_grad * up_pre * sigmoid_val * (1.0 + gate_pre * (1.0 - sigmoid_val))).astype(jnp.bfloat16)
    up_pre_grad = (act_grad * gate_pre * sigmoid_val).astype(jnp.bfloat16)
    gate_grad = lax.dot_general(rows_in, gate_pre_grad, contract_rows, preferred_element_type=jnp.float32)
    up_grad = lax.dot_general(rows_in, up_pre_grad, contract_rows, preferred_element_type=jnp.float32)
    input_grad = lax.dot_general(gate_pre_grad, gate_mat, contract_cols, preferred_element_type=jnp.float32)
    input_grad = input_grad + lax.dot_general(up_pre_grad, up_mat, contract_cols, preferred_element_type=jnp.float32)
    return (gate_grad, up_grad, down_grad, input_grad)

def reference(tokens, norm_gain, cotangent, routes, route_weight, gate_weight, up_weight, down_weight, scan_input, out_gate, step_size, decay_rate, write_keys, read_keys, start_state, out_proj):
    hidden = tokens.astype(jnp.float32)
    inverse = lax.rsqrt(lax.optimization_barrier(jnp.mean(hidden * hidden, axis=1)) + EPS)
    normed = (hidden * inverse[:, None] * norm_gain[None, :]).astype(jnp.bfloat16)
    most_rows = N_SP * CAP
    gate_whole = jnp.transpose(gate_weight.reshape(EXPERTS, 2, D, FF_HALF), (0, 2, 1, 3)).reshape(EXPERTS, D, FF)
    up_whole = jnp.transpose(up_weight.reshape(EXPERTS, 2, D, FF_HALF), (0, 2, 1, 3)).reshape(EXPERTS, D, FF)
    down_whole = down_weight.reshape(EXPERTS, FF, D)

    def expert_step(running, operands):
        expert_index, gate_mat, up_mat, down_mat = operands
        chosen = routes == expert_index
        scaling = lax.optimization_barrier(jnp.sum(jnp.where(chosen, route_weight, 0.0), axis=1))
        picked = jnp.any(chosen, axis=1)
        row_ids = jnp.nonzero(picked, size=most_rows, fill_value=0)[0]
        filled = jnp.arange(most_rows) < jnp.sum(picked.astype(jnp.int32))
        rows_in = normed[row_ids]
        scaled = (scaling[row_ids][:, None] * cotangent[row_ids].astype(jnp.float32)).astype(jnp.bfloat16)
        rows_cot = jnp.where(filled[:, None], scaled, jnp.zeros((), jnp.bfloat16))
        gate_grad, up_grad, down_grad, input_grad = expert_grads(rows_in, rows_cot, gate_mat, up_mat, down_mat)
        running = running.at[row_ids].add(jnp.where(filled[:, None], input_grad, 0.0))
        return (running, (gate_grad.astype(jnp.bfloat16), up_grad.astype(jnp.bfloat16), down_grad.astype(jnp.bfloat16)))
    normed_grad, (gate_all, up_all, down_all) = lax.scan(expert_step, jnp.zeros((TOKENS, D), jnp.float32), (jnp.arange(EXPERTS).astype(jnp.int32), gate_whole, up_whole, down_whole))
    gate_weight_grad = jnp.transpose(gate_all.reshape(EXPERTS, D, 2, FF_HALF), (0, 2, 1, 3)).reshape(N_SP, D, FF_HALF)
    up_weight_grad = jnp.transpose(up_all.reshape(EXPERTS, D, 2, FF_HALF), (0, 2, 1, 3)).reshape(N_SP, D, FF_HALF)
    down_weight_grad = down_all.reshape(N_SP, FF_HALF, D)
    gained = norm_gain[None, :] * normed_grad
    dotted = lax.optimization_barrier(jnp.sum(hidden * gained, axis=1))
    residual = cotangent.astype(jnp.float32) + inverse[:, None] * gained - hidden * (inverse ** 3 * dotted / D)[:, None]
    residual_grad = residual.astype(jnp.bfloat16)
    mix_grad = jnp.dot(residual_grad, out_proj, preferred_element_type=jnp.float32)
    per_group = HEADS // GROUPS
    scan_blocks = scan_input.reshape(BLOCKS, TOK_DEV, MIX)
    gate_blocks = out_gate.reshape(BLOCKS, TOK_DEV, MIX)
    step_blocks = jnp.transpose(step_size.reshape(HEADS, BLOCKS, TOK_DEV), (1, 0, 2))
    write_blocks = write_keys.reshape(BLOCKS, TOK_DEV, GROUPS * STATE)
    read_blocks = read_keys.reshape(BLOCKS, TOK_DEV, GROUPS * STATE)
    mix_blocks = mix_grad.reshape(BLOCKS, TOK_DEV, MIX)

    def forward_one(operands):
        scan_rows, gate_rows, step_rows, write_rows, read_rows, entry_state, mix_rows = operands
        return block_forward(scan_rows, gate_rows, step_rows, write_rows, read_rows, decay_rate, entry_state, mix_rows, per_group)
    gated, gate_grads, decays, carries, state_grads = lax.map(forward_one, (scan_blocks, gate_blocks, step_blocks, write_blocks, read_blocks, start_state, mix_blocks))

    def back_step(later_state, operands):
        decay_now, carry_now = operands
        return (carry_now + decay_now[:, None, None] * later_state, later_state)
    _, later_all = lax.scan(back_step, jnp.zeros((HEADS, HEAD_DIM, STATE), jnp.float32), (decays, carries), reverse=True)

    def back_one(operands):
        scan_rows, step_rows, write_rows, read_rows, entry_state, state_grad, later_state = operands
        return block_back(scan_rows, step_rows, write_rows, read_rows, decay_rate, entry_state, state_grad, later_state, per_group)
    scan_grads, write_grads, read_grads = lax.map(back_one, (scan_blocks, step_blocks, write_blocks, read_blocks, start_state, state_grads, later_all))
    gated_all = gated.reshape(TOKENS, MIX)
    out_proj_grad = jnp.dot(jnp.transpose(residual_grad), gated_all, preferred_element_type=jnp.float32)
    return (residual_grad, gate_weight_grad, up_weight_grad, down_weight_grad, out_proj_grad, scan_grads.reshape(TOKENS, MIX), gate_grads.reshape(TOKENS, MIX), write_grads.reshape(TOKENS, GROUPS * STATE), read_grads.reshape(TOKENS, GROUPS * STATE))
```

```python
import functools

import jax
import jax.numpy as jnp
from jax import lax
from jax.experimental import pallas as pl
from jax.experimental.pallas import tpu as pltpu
from jax.sharding import PartitionSpec as P

D = 2048
HEADS = 16
STATE = 64
GROUPS = 4


EPS = 1e-06
HIGHEST = lax.Precision.HIGHEST


def swapped(value, axis, apart):
    mask = 2**apart
    pairs = [(source, source ^ mask) for source in range(lax.axis_size(axis))]
    return lax.ppermute(value, axis, pairs)


def prefix(part, axis, combine, identity):
    count = lax.axis_size(axis)
    place = lax.axis_index(axis)
    ahead = count - 1 - place
    gathered = jax.tree.map(lambda a: lax.all_gather(a, axis), part)
    state = jax.tree.map(lambda a, e: jnp.zeros_like(a) + jnp.asarray(e, a.dtype), part, identity)

    def one(hop, state):
        source = count - 1 - hop
        return combine(
            state, jax.tree.map(lambda a: lax.dynamic_index_in_dim(a, source, 0, False), gathered)
        )

    return lax.fori_loop(0, ahead, one, state)


def prepare(scan_rows, step_rows, write_rows, read_rows, decay_rates, per_group):
    length = scan_rows.shape[0]
    head_count = step_rows.shape[0]
    logdec = jnp.cumsum(-decay_rates[:, None] * step_rows, axis=1)
    causal = jnp.arange(length)[:, None] >= jnp.arange(length)[None, :]
    spread = jnp.where(causal[None, :, :], logdec[:, :, None] - logdec[:, None, :], -jnp.inf)
    weights = jnp.exp(spread)
    inputs = (
        scan_rows.astype(jnp.float32).reshape(length, head_count, -1)
        * jnp.transpose(step_rows)[:, :, None]
    )
    write_head = jnp.repeat(
        write_rows.astype(jnp.float32).reshape(length, -1, STATE), per_group, axis=1
    )
    read_head = jnp.repeat(
        read_rows.astype(jnp.float32).reshape(length, -1, STATE), per_group, axis=1
    )
    scores = jnp.einsum("thn,shn->hts", read_head, write_head, precision=HIGHEST) * weights
    return (logdec, weights, inputs, write_head, read_head, scores)


def block_forward(
    scan_rows,
    gate_rows,
    step_rows,
    write_rows,
    read_rows,
    decay_rates,
    entry_state,
    mix_grad,
    per_group,
):
    logdec, weights, inputs, write_head, read_head, scores = prepare(
        scan_rows, step_rows, write_rows, read_rows, decay_rates, per_group
    )
    length, head_count = (inputs.shape[0], inputs.shape[1])
    growth = jnp.transpose(jnp.exp(logdec))
    output = jnp.einsum("hts,shp->thp", scores, inputs, precision=HIGHEST)
    output = output + growth[:, :, None] * jnp.einsum(
        "thn,hpn->thp", read_head, entry_state, precision=HIGHEST
    )
    gate_val = gate_rows.astype(jnp.float32).reshape(length, head_count, -1)
    sigmoid_val = jax.nn.sigmoid(gate_val)
    gated = (output * gate_val * sigmoid_val).reshape(length, -1).astype(jnp.bfloat16)
    out_grad = mix_grad.reshape(length, head_count, -1)
    state_grad = out_grad * gate_val * sigmoid_val
    gate_grad = (
        (out_grad * output * sigmoid_val * (1.0 + gate_val * (1.0 - sigmoid_val)))
        .reshape(length, -1)
        .astype(jnp.bfloat16)
    )
    carried = jnp.einsum("th,thp,thn->hpn", growth, state_grad, read_head, precision=HIGHEST)
    return (gated, gate_grad, jnp.exp(logdec[:, -1]), carried, state_grad)


def block_back(
    scan_rows,
    step_rows,
    write_rows,
    read_rows,
    decay_rates,
    entry_state,
    state_grad,
    later_state,
    per_group,
):
    logdec, weights, inputs, write_head, read_head, scores = prepare(
        scan_rows, step_rows, write_rows, read_rows, decay_rates, per_group
    )
    length, head_count = (inputs.shape[0], inputs.shape[1])
    growth = jnp.transpose(jnp.exp(logdec))
    shrink = jnp.transpose(jnp.exp(logdec[:, -1:] - logdec))
    in_grad = jnp.einsum("hts,thp->shp", scores, state_grad, precision=HIGHEST)
    in_grad = in_grad + shrink[:, :, None] * jnp.einsum(
        "shn,hpn->shp", write_head, later_state, precision=HIGHEST
    )
    scan_grad = (
        (in_grad * jnp.transpose(step_rows)[:, :, None]).reshape(length, -1).astype(jnp.bfloat16)
    )
    pair_terms = jnp.einsum("thp,shp->hts", state_grad, inputs, precision=HIGHEST) * weights
    read_grad = jnp.einsum("hts,shn->thn", pair_terms, write_head, precision=HIGHEST)
    read_grad = read_grad + growth[:, :, None] * jnp.einsum(
        "thp,hpn->thn", state_grad, entry_state, precision=HIGHEST
    )
    write_grad = jnp.einsum("hts,thn->shn", pair_terms, read_head, precision=HIGHEST)
    write_grad = write_grad + shrink[:, :, None] * jnp.einsum(
        "shp,hpn->shn", inputs, later_state, precision=HIGHEST
    )
    group_count = head_count // per_group
    read_total = (
        jnp.sum(read_grad.reshape(length, group_count, per_group, -1), axis=2)
        .reshape(length, -1)
        .astype(jnp.bfloat16)
    )
    write_total = (
        jnp.sum(write_grad.reshape(length, group_count, per_group, -1), axis=2)
        .reshape(length, -1)
        .astype(jnp.bfloat16)
    )
    return (scan_grad, write_total, read_total)


def expert_grads(rows_in, rows_cot, gate_mat, up_mat, down_mat):
    contract_rows = (((0,), (0,)), ((), ()))
    contract_cols = (((1,), (1,)), ((), ()))
    gate_pre = jnp.dot(rows_in, gate_mat, preferred_element_type=jnp.float32)
    up_pre = jnp.dot(rows_in, up_mat, preferred_element_type=jnp.float32)
    sigmoid_val = jax.nn.sigmoid(gate_pre)
    active = (gate_pre * sigmoid_val * up_pre).astype(jnp.bfloat16)
    down_grad = lax.dot_general(active, rows_cot, contract_rows, preferred_element_type=jnp.float32)
    act_grad = lax.dot_general(
        rows_cot, down_mat, contract_cols, preferred_element_type=jnp.float32
    )
    gate_pre_grad = (
        act_grad * up_pre * sigmoid_val * (1.0 + gate_pre * (1.0 - sigmoid_val))
    ).astype(jnp.bfloat16)
    up_pre_grad = (act_grad * gate_pre * sigmoid_val).astype(jnp.bfloat16)
    gate_grad = lax.dot_general(
        rows_in, gate_pre_grad, contract_rows, preferred_element_type=jnp.float32
    )
    up_grad = lax.dot_general(
        rows_in, up_pre_grad, contract_rows, preferred_element_type=jnp.float32
    )
    input_grad = lax.dot_general(
        gate_pre_grad, gate_mat, contract_cols, preferred_element_type=jnp.float32
    )
    input_grad = input_grad + lax.dot_general(
        up_pre_grad, up_mat, contract_cols, preferred_element_type=jnp.float32
    )
    return (gate_grad, up_grad, down_grad, input_grad)


def compose(higher, nearer):
    return (nearer[0] * higher[0], nearer[1] + nearer[0][:, None, None] * higher[1])


MESH = pl.DeviceIdType.MESH


def remote(src, dst, send, recv, device):
    return pltpu.make_async_remote_copy(
        src_ref=src,
        dst_ref=dst,
        send_sem=send,
        recv_sem=recv,
        device_id=device,
        device_id_type=MESH,
    )


def greet(devices):
    barrier = pltpu.get_barrier_semaphore()
    for device in devices:
        pl.semaphore_signal(barrier, inc=1, device_id=device, device_id_type=MESH)
    pl.semaphore_wait(barrier, len(devices))


def gather_kernel(
    nz, a_ref, b_ref, w_ref, oa_ref, ob_ref, ow_ref, own_sem, z_send, z_recv, x_sem, y_sem, c_sem, d_sem, w_sem
):
    rows = a_ref.shape[0]
    part = rows // 4
    sp, tp = lax.axis_index("sp"), lax.axis_index("tp")
    z, x, y, c = sp // 2, sp % 2, tp // 2, tp % 2
    count = 2 * nz
    over_x = (z * 2 + 1 - x, tp)
    over_y = (sp, (1 - y) * 2 + c)
    over_c = (sp, y * 2 + 1 - c)
    peers = [((sp + k) % count, tp) for k in range(1, count)]
    greet(peers + [over_y, over_c])

    def span(core, row, whole):
        if whole:
            return core * (2 * part), 2 * part
        return core * (2 * part) + row * part, part

    def copies(block, piece, send, recv, device, own=False):
        start, size = piece
        made = []
        for k, (src, dst) in enumerate(((a_ref, oa_ref), (b_ref, ob_ref))):
            at = pl.ds(pl.multiple_of(block * rows + start, part), size)
            source = src.at[pl.ds(pl.multiple_of(start, part), size)] if own else dst.at[at]
            made.append(remote(source, dst.at[at], send.at[k, block], recv.at[k, block], device))
        return made

    def go(made):
        for copy in made:
            copy.start()

    def arrived(made):
        for copy in made:
            copy.wait_recv()

    def sent(made):
        for copy in made:
            copy.wait_send()

    mine_half = span(c, y, True)
    mine_part = span(c, y, False)
    y_part = span(c, 1 - y, False)
    for k in range(1, count):
        other = ((sp + k) % count, tp)
        remote(w_ref, ow_ref.at[sp], w_sem.at[0, k], w_sem.at[1, k], other).start()
    steps = []

    def send_if(condition, make):
        if condition is None:
            go(make())
        else:
            @pl.when(condition)
            def _():
                go(make())
        steps.append((condition, make))

    up = (jnp.minimum(z + 1, nz - 1) * 2 + x, tp)
    down = (jnp.maximum(z - 1, 0) * 2 + x, tp)
    own = z * 2 + x
    send_if(z < nz - 1, lambda: copies(own, mine_half, z_send.at[0], z_recv, up, True))
    send_if(z > 0, lambda: copies(own, mine_half, z_send.at[1], z_recv, down, True))
    send_if(None, lambda: copies(own, mine_half, x_sem.at[0], x_sem.at[1], over_x, True))
    locals_ = [
        pltpu.make_async_copy(src, dst.at[pl.ds(pl.multiple_of(own * rows, rows), rows)], own_sem.at[k])
        for k, (src, dst) in enumerate(((a_ref, oa_ref), (b_ref, ob_ref)))
    ]
    locals_.append(pltpu.make_async_copy(w_ref, ow_ref.at[sp], own_sem.at[2]))
    go(locals_)

    def sides(step):
        if step == 0:
            return [(None, z, 0)]
        return [(z - step >= 0, z - step, 0), (z + step <= nz - 1, z + step, 1)]

    def guarded(condition, work):
        if condition is None:
            work()
        else:
            pl.when(condition)(work)

    def from_z(step):
        for condition, at, way in sides(step):
            block = at * 2 + x
            piece = mine_half if step == 1 else mine_part
            guarded(condition, lambda: arrived(copies(block, piece, z_send.at[way], z_recv, up)))
            onward = jnp.logical_and(condition, z < nz - 1 if way == 0 else z > 0)
            target = up if way == 0 else down
            send_if(
                onward,
                lambda block=block, way=way, target=target: copies(
                    block, mine_part, z_send.at[way], z_recv, target
                ),
            )
            send_if(
                condition,
                lambda block=block: copies(block, mine_part, x_sem.at[0], x_sem.at[1], over_x),
            )
            if step >= 2:
                send_if(
                    condition,
                    lambda block=block: copies(block, mine_part, y_sem.at[0], y_sem.at[1], over_y),
                )
            send_if(
                condition,
                lambda block=block, piece=piece: copies(
                    block, piece, c_sem.at[0], c_sem.at[1], over_c
                ),
            )

    def from_x(step):
        for condition, at, way in sides(step):
            block = at * 2 + 1 - x
            piece = mine_half if step == 0 else mine_part
            guarded(
                condition,
                lambda: arrived(copies(block, piece, x_sem.at[0], x_sem.at[1], over_x)),
            )
            if step >= 1:
                send_if(
                    condition,
                    lambda block=block: copies(block, mine_part, y_sem.at[0], y_sem.at[1], over_y),
                )
            send_if(
                condition,
                lambda block=block, piece=piece: copies(
                    block, piece, c_sem.at[0], c_sem.at[1], over_c
                ),
            )

    def from_y(step, column):
        for condition, at, way in sides(step):
            block = at * 2 + column
            guarded(
                condition,
                lambda: arrived(copies(block, y_part, y_sem.at[0], y_sem.at[1], over_y)),
            )
            send_if(
                condition,
                lambda block=block: copies(block, y_part, d_sem.at[0], d_sem.at[1], over_c),
            )

    for step in range(nz + 2):
        if 1 <= step < nz:
            from_z(step)
        if 0 <= step - 1 < nz:
            from_x(step - 1)
        if 2 <= step - 1 < nz:
            from_y(step - 1, x)
        if 1 <= step - 2 < nz:
            from_y(step - 2, 1 - x)

    for step in range(nz):
        for condition, at, way in sides(step):
            for column, first, then in ((x, 1, 2), (1 - x, 0, 1)):
                block = at * 2 + column
                if step >= first:
                    piece = span(1 - c, y, step == first)
                    guarded(
                        condition,
                        lambda: arrived(copies(block, piece, c_sem.at[0], c_sem.at[1], over_c)),
                    )
                if step >= then:
                    piece = span(1 - c, 1 - y, False)
                    guarded(
                        condition,
                        lambda: arrived(copies(block, piece, d_sem.at[0], d_sem.at[1], over_c)),
                    )
    for k in range(1, count):
        source = (sp + count - k) % count
        remote(w_ref, ow_ref.at[source], w_sem.at[0, k], w_sem.at[1, k], over_x).wait_recv()
    for k in range(1, count):
        remote(w_ref, ow_ref.at[sp], w_sem.at[0, k], w_sem.at[1, k], over_x).wait_send()
    for condition, make in steps:
        guarded(condition, lambda: sent(make()))
    for copy in locals_:
        copy.wait()


def gather_rows(nz, first, second, weights):
    count = 2 * nz
    rows, width = first.shape
    dma = pltpu.SemaphoreType.DMA
    whole = jax.ShapeDtypeStruct((count * rows, width), first.dtype)
    return pl.pallas_call(
        functools.partial(gather_kernel, nz),
        out_shape=(whole, whole, jax.ShapeDtypeStruct((count,) + weights.shape, weights.dtype)),
        in_specs=[pl.BlockSpec(memory_space=pltpu.VMEM)] * 3,
        out_specs=(pl.BlockSpec(memory_space=pl.ANY),) * 3,
        scratch_shapes=[
            dma((3,)),
            dma((2, 2, count)),
            dma((2, count)),
            dma((2, 2, count)),
            dma((2, 2, count)),
            dma((2, 2, count)),
            dma((2, 2, count)),
            dma((2, count)),
        ],
        compiler_params=pltpu.CompilerParams(collective_id=0, has_side_effects=True),
        name="gather_rows",
    )(first, second, weights)


def total_kernel(
    nz, p_ref, o_ref, rc, s1, ra, rb, sa, sb, r2, s3, rz, full, c_sem, m_sem, n_sem, z_sem, g_sem
):
    width = p_ref.shape[1]
    half, quarter = width // 2, width // 4
    rows = p_ref.shape[0] // (2 * nz)
    sp, tp = lax.axis_index("sp"), lax.axis_index("tp")
    z, x, y, c = sp // 2, sp % 2, tp // 2, tp % 2
    over_x = (z * 2 + 1 - x, tp)
    over_y = (sp, (1 - y) * 2 + c)
    over_c = (sp, y * 2 + 1 - c)
    f32, bf16 = jnp.float32, jnp.bfloat16
    greet([(((z + k) % nz) * 2 + x, tp) for k in range(1, nz)] + [over_x, over_y, over_c])

    def lanes(index, size):
        return pl.ds(pl.multiple_of(index * size, size), size)

    def plane(i):
        return (z + 1 + i) % nz

    made = []

    def core_copy(i):
        at = lanes(plane(i), 2 * rows)
        return remote(
            p_ref.at[at, lanes(1 - c, half)], rc.at[at], c_sem.at[0, i], c_sem.at[1, i], over_c
        )

    for i in range(nz):
        copy = core_copy(i)
        copy.start()
        made.append(copy)
    firsts, seconds = [], []
    for i in range(nz):
        made[i].wait_recv()
        at = lanes(plane(i), 2 * rows)
        s1[at] = (p_ref[at, lanes(c, half)].astype(f32) + rc[at].astype(f32)).astype(bf16)
        if i % 2 == 0:
            copy = remote(
                s1.at[at, lanes(1 - y, quarter)],
                ra.at[i // 2],
                m_sem.at[0, i],
                m_sem.at[1, i],
                over_y,
            )
        else:
            copy = remote(
                s1.at[lanes(plane(i) * 2 + 1 - x, rows)],
                rb.at[i // 2],
                m_sem.at[0, i],
                m_sem.at[1, i],
                over_x,
            )
        copy.start()
        firsts.append(copy)
    for i in range(nz):
        firsts[i].wait_recv()
        k = i // 2
        if i % 2 == 0:
            at = lanes(plane(i), 2 * rows)
            sa[k] = (s1[at, lanes(y, quarter)].astype(f32) + ra[k].astype(f32)).astype(bf16)
            copy = remote(
                sa.at[k, lanes(1 - x, rows)], r2.at[i], n_sem.at[0, i], n_sem.at[1, i], over_x
            )
        else:
            at = lanes(plane(i) * 2 + x, rows)
            sb[k] = (s1[at].astype(f32) + rb[k].astype(f32)).astype(bf16)
            copy = remote(
                sb.at[k, :, lanes(1 - y, quarter)],
                r2.at[i],
                n_sem.at[0, i],
                n_sem.at[1, i],
                over_y,
            )
        copy.start()
        seconds.append(copy)
    along = []
    total = None
    for i in range(nz):
        seconds[i].wait_recv()
        k = i // 2
        held = sa[k, lanes(x, rows)] if i % 2 == 0 else sb[k, :, lanes(y, quarter)]
        value = held.astype(f32) + r2[i].astype(f32)
        if i < nz - 1:
            s3[i] = value.astype(bf16)
            copy = remote(
                s3.at[i], rz.at[i], z_sem.at[0, i], z_sem.at[1, i], (plane(i) * 2 + x, tp)
            )
            copy.start()
            along.append(copy)
        else:
            total = value
    for i in range(nz - 1):
        along[i].wait_recv()
        total = total + rz[i].astype(f32)
    mine = c * 2 + y
    theirs = c * 2 + 1 - y
    full[:, lanes(mine, quarter)] = total.astype(bf16)
    own = full.at[:, lanes(mine, quarter)]
    to_y = remote(own, own, g_sem.at[0, 0], g_sem.at[1, 0], over_y)
    to_c = remote(own, own, g_sem.at[0, 1], g_sem.at[1, 1], over_c)
    to_y.start()
    to_c.start()
    to_y.wait_recv()
    got = full.at[:, lanes(theirs, quarter)]
    onward = remote(got, got, g_sem.at[0, 2], g_sem.at[1, 2], over_c)
    onward.start()
    to_c.wait_recv()
    onward.wait_recv()
    o_ref[...] = full[...]
    for copy in made + firsts + seconds + along + [to_y, to_c, onward]:
        copy.wait_send()


def total_rows(nz, parts):
    count = 2 * nz
    rows, width = parts.shape[0] // count, parts.shape[1]
    half, quarter = width // 2, width // 4
    evens, odds = (nz + 1) // 2, max(nz // 2, 1)
    dma = pltpu.SemaphoreType.DMA
    vmem = functools.partial(pltpu.VMEM, dtype=jnp.bfloat16)
    return pl.pallas_call(
        functools.partial(total_kernel, nz),
        out_shape=jax.ShapeDtypeStruct((rows, width), jnp.bfloat16),
        in_specs=[pl.BlockSpec(memory_space=pltpu.VMEM)],
        out_specs=pl.BlockSpec(memory_space=pltpu.VMEM),
        scratch_shapes=[
            vmem((count * rows, half)),
            vmem((count * rows, half)),
            vmem((evens, 2 * rows, quarter)),
            vmem((odds, rows, half)),
            vmem((evens, 2 * rows, quarter)),
            vmem((odds, rows, half)),
            vmem((nz, rows, quarter)),
            vmem((nz, rows, quarter)),
            vmem((nz, rows, quarter)),
            vmem((rows, width)),
            dma((2, nz)),
            dma((2, nz)),
            dma((2, nz)),
            dma((2, nz)),
            dma((2, 3)),
        ],
        compiler_params=pltpu.CompilerParams(collective_id=1, has_side_effects=True),
        name="total_rows",
    )(parts)


def dense_grads(normed, cotangent, routes, route_weight, gate_mat, up_mat, down_mat):
    sp_count = lax.axis_size("sp")
    experts_count = sp_count // 2
    nz = sp_count // 2
    names = jnp.arange(experts_count, dtype=jnp.int32)[:, None]
    table = jnp.where(routes[None, :, 0] == names, route_weight[None, :, 0], 0.0)
    table = table + jnp.where(routes[None, :, 1] == names, route_weight[None, :, 1], 0.0)
    rows_in, cot_all, tables = gather_rows(nz, normed, cotangent, table)
    weight_all = lax.dynamic_index_in_dim(tables, lax.axis_index("sp") // 2, 1, False).reshape(-1)
    rows_cot = (weight_all[:, None] * cot_all.astype(jnp.float32)).astype(jnp.bfloat16)
    gate_grad, up_grad, down_grad, input_part = expert_grads(
        rows_in, rows_cot, gate_mat, up_mat, down_mat
    )
    normed_grad = total_rows(nz, input_part.astype(jnp.bfloat16)).astype(jnp.float32)
    return gate_grad, up_grad, down_grad, normed_grad


def routed_grads(normed, cotangent, routes, route_weight, gate_mat, up_mat, down_mat):
    sp_count = lax.axis_size("sp")
    tp_count = lax.axis_size("tp")
    tok_rows = normed.shape[0]
    experts_count = sp_count // 2
    capacity = min(tok_rows, 4 * tok_rows // experts_count)
    quarter = D // tp_count
    route_flat = routes.reshape(-1)
    member = (route_flat[:, None] == jnp.arange(experts_count, dtype=jnp.int32)[None, :]).astype(
        jnp.int32
    )
    earlier_count = jnp.sum((jnp.cumsum(member, axis=0) - member) * member, axis=1)
    places = (route_flat * capacity + earlier_count).reshape(tok_rows, 2)
    slot_ids = jnp.arange(experts_count * capacity, dtype=jnp.int32)[:, None]
    first_hit = slot_ids == places[None, :, 0]
    second_hit = slot_ids == places[None, :, 1]
    placing = jnp.logical_or(first_hit, second_hit)
    place_matrix = placing.astype(jnp.bfloat16)
    slot_weight = jnp.sum(
        jnp.where(first_hit, route_weight[None, :, 0], 0.0)
        + jnp.where(second_hit, route_weight[None, :, 1], 0.0),
        axis=1,
    )
    send_in = jnp.dot(place_matrix, normed, preferred_element_type=jnp.float32).astype(jnp.bfloat16)
    send_cot = (
        slot_weight[:, None] * jnp.dot(place_matrix, cotangent, preferred_element_type=jnp.float32)
    ).astype(jnp.bfloat16)
    half_cap = capacity // 2
    part_in, part_cot = (
        lax.all_to_all(
            send_in.reshape(sp_count, half_cap, D), "sp", split_axis=0, concat_axis=0, tiled=True
        ),
        lax.all_to_all(
            send_cot.reshape(sp_count, half_cap, D), "sp", split_axis=0, concat_axis=0, tiled=True
        ),
    )
    other_in, other_cot = swapped((part_in, part_cot), "sp", 0)
    lower_bit = lax.axis_index("sp") % 2 == 0
    recv_in = jnp.concatenate(
        [jnp.where(lower_bit, part_in, other_in), jnp.where(lower_bit, other_in, part_in)], axis=1
    )
    recv_cot = jnp.concatenate(
        [jnp.where(lower_bit, part_cot, other_cot), jnp.where(lower_bit, other_cot, part_cot)],
        axis=1,
    )
    rows_in = recv_in.reshape(-1, D)
    rows_cot = recv_cot.reshape(-1, D)
    gate_grad, up_grad, down_grad, input_part = expert_grads(
        rows_in, rows_cot, gate_mat, up_mat, down_mat
    )
    input_quarter = lax.psum_scatter(input_part, "tp", scatter_dimension=1, tiled=True)
    returned = lax.all_to_all(
        input_quarter.reshape(sp_count, capacity, quarter),
        "sp",
        split_axis=0,
        concat_axis=0,
        tiled=True,
    )
    pair_total = jnp.sum(returned.reshape(experts_count, 2, capacity, quarter), axis=1).reshape(
        -1, quarter
    )
    token_quarter = lax.dot_general(
        placing.astype(jnp.float32), pair_total, (((0,), (0,)), ((), ())), precision=HIGHEST
    )
    normed_grad = lax.all_gather(token_quarter, "tp", axis=1, tiled=True)
    return gate_grad, up_grad, down_grad, normed_grad


def shards(
    tokens,
    norm_gain,
    cotangent,
    routes,
    route_weight,
    gate_weight,
    up_weight,
    down_weight,
    scan_input,
    out_gate,
    step_size,
    decay_rate,
    write_keys,
    read_keys,
    start_state,
    out_proj,
):
    sp_count = lax.axis_size("sp")
    tp_count = lax.axis_size("tp")
    tok_rows = tokens.shape[0]
    experts_count = sp_count // 2
    capacity = min(tok_rows, 4 * tok_rows // experts_count)
    quarter = D // tp_count
    hidden = tokens.astype(jnp.float32)
    inverse = lax.rsqrt(jnp.mean(hidden * hidden, axis=1) + EPS)
    normed = (hidden * inverse[:, None] * norm_gain[None, :]).astype(jnp.bfloat16)
    work = dense_grads if capacity == tok_rows and tp_count == 4 else routed_grads
    gate_grad, up_grad, down_grad, normed_grad = work(
        normed, cotangent, routes, route_weight, gate_weight[0], up_weight[0], down_weight[0]
    )
    gained = norm_gain[None, :] * normed_grad
    dotted = jnp.sum(hidden * gained, axis=1)
    residual = (
        cotangent.astype(jnp.float32)
        + inverse[:, None] * gained
        - hidden * (inverse**3 * dotted / D)[:, None]
    )
    residual_grad = residual.astype(jnp.bfloat16)
    mix_grad = jnp.dot(residual_grad, out_proj, preferred_element_type=jnp.float32)
    per_group = HEADS // GROUPS
    gated, gate_out_grad, decay_now, carried, state_grad = block_forward(
        scan_input,
        out_gate,
        step_size,
        write_keys,
        read_keys,
        decay_rate,
        start_state[0],
        mix_grad,
        per_group,
    )
    totals, later_state = prefix(
        (decay_now, carried), "sp", compose, (jnp.ones_like(decay_now), jnp.zeros_like(carried))
    )
    scan_grad, write_grad, read_grad = block_back(
        scan_input,
        step_size,
        write_keys,
        read_keys,
        decay_rate,
        start_state[0],
        state_grad,
        later_state,
        per_group,
    )
    out_proj_grad = lax.psum_scatter(
        lax.dot_general(
            residual_grad, gated, (((0,), (0,)), ((), ())), preferred_element_type=jnp.float32
        ),
        "sp",
        scatter_dimension=0,
        tiled=True,
    )
    residual_part = lax.dynamic_slice_in_dim(
        residual_grad, lax.axis_index("tp") * quarter, quarter, 1
    )
    return (
        residual_part,
        gate_grad.astype(jnp.bfloat16)[None],
        up_grad.astype(jnp.bfloat16)[None],
        down_grad.astype(jnp.bfloat16)[None],
        out_proj_grad,
        scan_grad,
        gate_out_grad,
        write_grad,
        read_grad,
    )


def solution(mesh):
    return jax.shard_map(
        shards,
        mesh=mesh,
        in_specs=(
            P("sp", None),
            P(),
            P("sp", None),
            P("sp", None),
            P("sp", None),
            P("sp", None, "tp"),
            P("sp", None, "tp"),
            P("sp", "tp", None),
            P("sp", "tp"),
            P("sp", "tp"),
            P("tp", "sp"),
            P("tp"),
            P("sp", "tp"),
            P("sp", "tp"),
            P("sp", "tp", None, None),
            P(None, "tp"),
        ),
        out_specs=(
            P("sp", "tp"),
            P("sp", None, "tp"),
            P("sp", None, "tp"),
            P("sp", "tp", None),
            P("sp", "tp"),
            P("sp", "tp"),
            P("sp", "tp"),
            P("sp", "tp"),
            P("sp", "tp"),
        ),
        check_vma=False,
    )
```

```python
import functools

import jax
import jax.numpy as jnp
from jax import lax
from jax.experimental import pallas as pl
from jax.experimental.pallas import tpu as pltpu
from jax.sharding import PartitionSpec as P

D = 2048
HEADS = 16
STATE = 64
GROUPS = 4


EPS = 1e-06
HIGHEST = lax.Precision.HIGHEST


def swapped(value, axis, apart):
    mask = 2**apart
    pairs = [(source, source ^ mask) for source in range(lax.axis_size(axis))]
    return lax.ppermute(value, axis, pairs)


def prefix(part, axis, combine, identity):
    count = lax.axis_size(axis)
    place = lax.axis_index(axis)
    ahead = count - 1 - place
    gathered = jax.tree.map(lambda a: lax.all_gather(a, axis), part)
    state = jax.tree.map(lambda a, e: jnp.zeros_like(a) + jnp.asarray(e, a.dtype), part, identity)

    def one(hop, state):
        source = count - 1 - hop
        return combine(
            state, jax.tree.map(lambda a: lax.dynamic_index_in_dim(a, source, 0, False), gathered)
        )

    return lax.fori_loop(0, ahead, one, state)


def prepare(scan_rows, step_rows, write_rows, read_rows, decay_rates, per_group):
    length = scan_rows.shape[0]
    head_count = step_rows.shape[0]
    logdec = jnp.cumsum(-decay_rates[:, None] * step_rows, axis=1)
    causal = jnp.arange(length)[:, None] >= jnp.arange(length)[None, :]
    spread = jnp.where(causal[None, :, :], logdec[:, :, None] - logdec[:, None, :], -jnp.inf)
    weights = jnp.exp(spread)
    inputs = (
        scan_rows.astype(jnp.float32).reshape(length, head_count, -1)
        * jnp.transpose(step_rows)[:, :, None]
    )
    write_head = jnp.repeat(
        write_rows.astype(jnp.float32).reshape(length, -1, STATE), per_group, axis=1
    )
    read_head = jnp.repeat(
        read_rows.astype(jnp.float32).reshape(length, -1, STATE), per_group, axis=1
    )
    scores = jnp.einsum("thn,shn->hts", read_head, write_head, precision=HIGHEST) * weights
    return (logdec, weights, inputs, write_head, read_head, scores)


def block_forward(
    scan_rows,
    gate_rows,
    step_rows,
    write_rows,
    read_rows,
    decay_rates,
    entry_state,
    mix_grad,
    per_group,
):
    logdec, weights, inputs, write_head, read_head, scores = prepare(
        scan_rows, step_rows, write_rows, read_rows, decay_rates, per_group
    )
    length, head_count = (inputs.shape[0], inputs.shape[1])
    growth = jnp.transpose(jnp.exp(logdec))
    output = jnp.einsum("hts,shp->thp", scores, inputs, precision=HIGHEST)
    output = output + growth[:, :, None] * jnp.einsum(
        "thn,hpn->thp", read_head, entry_state, precision=HIGHEST
    )
    gate_val = gate_rows.astype(jnp.float32).reshape(length, head_count, -1)
    sigmoid_val = jax.nn.sigmoid(gate_val)
    gated = (output * gate_val * sigmoid_val).reshape(length, -1).astype(jnp.bfloat16)
    out_grad = mix_grad.reshape(length, head_count, -1)
    state_grad = out_grad * gate_val * sigmoid_val
    gate_grad = (
        (out_grad * output * sigmoid_val * (1.0 + gate_val * (1.0 - sigmoid_val)))
        .reshape(length, -1)
        .astype(jnp.bfloat16)
    )
    carried = jnp.einsum("th,thp,thn->hpn", growth, state_grad, read_head, precision=HIGHEST)
    return (gated, gate_grad, jnp.exp(logdec[:, -1]), carried, state_grad)


def block_back(
    scan_rows,
    step_rows,
    write_rows,
    read_rows,
    decay_rates,
    entry_state,
    state_grad,
    later_state,
    per_group,
):
    logdec, weights, inputs, write_head, read_head, scores = prepare(
        scan_rows, step_rows, write_rows, read_rows, decay_rates, per_group
    )
    length, head_count = (inputs.shape[0], inputs.shape[1])
    growth = jnp.transpose(jnp.exp(logdec))
    shrink = jnp.transpose(jnp.exp(logdec[:, -1:] - logdec))
    in_grad = jnp.einsum("hts,thp->shp", scores, state_grad, precision=HIGHEST)
    in_grad = in_grad + shrink[:, :, None] * jnp.einsum(
        "shn,hpn->shp", write_head, later_state, precision=HIGHEST
    )
    scan_grad = (
        (in_grad * jnp.transpose(step_rows)[:, :, None]).reshape(length, -1).astype(jnp.bfloat16)
    )
    pair_terms = jnp.einsum("thp,shp->hts", state_grad, inputs, precision=HIGHEST) * weights
    read_grad = jnp.einsum("hts,shn->thn", pair_terms, write_head, precision=HIGHEST)
    read_grad = read_grad + growth[:, :, None] * jnp.einsum(
        "thp,hpn->thn", state_grad, entry_state, precision=HIGHEST
    )
    write_grad = jnp.einsum("hts,thn->shn", pair_terms, read_head, precision=HIGHEST)
    write_grad = write_grad + shrink[:, :, None] * jnp.einsum(
        "shp,hpn->shn", inputs, later_state, precision=HIGHEST
    )
    group_count = head_count // per_group
    read_total = (
        jnp.sum(read_grad.reshape(length, group_count, per_group, -1), axis=2)
        .reshape(length, -1)
        .astype(jnp.bfloat16)
    )
    write_total = (
        jnp.sum(write_grad.reshape(length, group_count, per_group, -1), axis=2)
        .reshape(length, -1)
        .astype(jnp.bfloat16)
    )
    return (scan_grad, write_total, read_total)


def expert_grads(rows_in, rows_cot, gate_mat, up_mat, down_mat):
    contract_rows = (((0,), (0,)), ((), ()))
    contract_cols = (((1,), (1,)), ((), ()))
    gate_pre = jnp.dot(rows_in, gate_mat, preferred_element_type=jnp.float32)
    up_pre = jnp.dot(rows_in, up_mat, preferred_element_type=jnp.float32)
    sigmoid_val = jax.nn.sigmoid(gate_pre)
    active = (gate_pre * sigmoid_val * up_pre).astype(jnp.bfloat16)
    down_grad = lax.dot_general(active, rows_cot, contract_rows, preferred_element_type=jnp.float32)
    act_grad = lax.dot_general(
        rows_cot, down_mat, contract_cols, preferred_element_type=jnp.float32
    )
    gate_pre_grad = (
        act_grad * up_pre * sigmoid_val * (1.0 + gate_pre * (1.0 - sigmoid_val))
    ).astype(jnp.bfloat16)
    up_pre_grad = (act_grad * gate_pre * sigmoid_val).astype(jnp.bfloat16)
    gate_grad = lax.dot_general(
        rows_in, gate_pre_grad, contract_rows, preferred_element_type=jnp.float32
    )
    up_grad = lax.dot_general(
        rows_in, up_pre_grad, contract_rows, preferred_element_type=jnp.float32
    )
    input_grad = lax.dot_general(
        gate_pre_grad, gate_mat, contract_cols, preferred_element_type=jnp.float32
    )
    input_grad = input_grad + lax.dot_general(
        up_pre_grad, up_mat, contract_cols, preferred_element_type=jnp.float32
    )
    return (gate_grad, up_grad, down_grad, input_grad)


def compose(higher, nearer):
    return (nearer[0] * higher[0], nearer[1] + nearer[0][:, None, None] * higher[1])


MESH = pl.DeviceIdType.MESH


def remote(src, dst, send, recv, device):
    return pltpu.make_async_remote_copy(
        src_ref=src,
        dst_ref=dst,
        send_sem=send,
        recv_sem=recv,
        device_id=device,
        device_id_type=MESH,
    )


def greet(devices):
    barrier = pltpu.get_barrier_semaphore()
    for device in devices:
        pl.semaphore_signal(barrier, inc=1, device_id=device, device_id_type=MESH)
    pl.semaphore_wait(barrier, len(devices))


def gather_kernel(
    nz,
    a_ref,
    b_ref,
    w_ref,
    oa_ref,
    ob_ref,
    ow_ref,
    own_sem,
    z_send,
    z_recv,
    x_sem,
    y_sem,
    c_sem,
    d_sem,
    w_sem,
):
    rows = a_ref.shape[0]
    part = rows // 4
    sp, tp = lax.axis_index("sp"), lax.axis_index("tp")
    z, x, y, c = sp // 2, sp % 2, tp // 2, tp % 2
    count = 2 * nz
    over_x = (z * 2 + 1 - x, tp)
    over_y = (sp, (1 - y) * 2 + c)
    over_c = (sp, y * 2 + 1 - c)
    peers = [((sp + k) % count, tp) for k in range(1, count)]
    greet(peers + [over_y, over_c])

    mine = (c * 2 + y) * part
    beside = (c * 2 + 1 - y) * part
    mine_other = ((1 - c) * 2 + y) * part
    beside_other = ((1 - c) * 2 + 1 - y) * part
    pairs = ((a_ref, oa_ref), (b_ref, ob_ref))
    own = z * 2 + x
    up = (jnp.minimum(z + 1, nz - 1) * 2 + x, tp)
    down = (jnp.maximum(z - 1, 0) * 2 + x, tp)
    sends = []

    def piece(k, block, start, sems, device):
        src, dst = pairs[k]
        at = dst.at[pl.ds(pl.multiple_of(block * rows + start, part), part)]
        source = at
        if block is own:
            source = src.at[pl.ds(pl.multiple_of(start, part), part)]
        return remote(source, at, sems[0].at[k, block], sems[1].at[k, block], device)

    def guarded(condition, work):
        if condition is None:
            work()
        else:
            pl.when(condition)(work)

    def send(condition, *what):
        guarded(condition, lambda: piece(*what).start())
        sends.append((condition, what))

    def take(condition, *what):
        guarded(condition, lambda: piece(*what).wait_recv())

    z_up, z_down = (z_send.at[0], z_recv.at[0]), (z_send.at[1], z_recv.at[0])
    z_up_late, z_down_late = (z_send.at[2], z_recv.at[1]), (z_send.at[3], z_recv.at[1])
    over_x_sems, over_x_late = (x_sem.at[0], x_sem.at[1]), (x_sem.at[2], x_sem.at[3])
    over_y_sems = (y_sem.at[0], y_sem.at[1])
    core_mine, core_beside = (c_sem.at[0], c_sem.at[1]), (d_sem.at[0], d_sem.at[1])
    for k in range(2):
        send(z < nz - 1, k, own, mine, z_up, up)
        send(z > 0, k, own, mine, z_down, down)
        send(None, k, own, mine, over_x_sems, over_x)
    for k in range(1, count):
        other = ((sp + k) % count, tp)
        remote(w_ref, ow_ref.at[sp], w_sem.at[0, k], w_sem.at[1, k], other).start()
    locals_ = [
        pltpu.make_async_copy(src, dst.at[pl.ds(pl.multiple_of(own * rows, rows), rows)], own_sem.at[k])
        for k, (src, dst) in enumerate(pairs)
    ]
    locals_.append(pltpu.make_async_copy(w_ref, ow_ref.at[sp], own_sem.at[2]))
    for copy in locals_:
        copy.start()

    def sides(step):
        if step == 0:
            return [(None, z, 0)]
        return [(z - step >= 0, z - step, 0), (z + step <= nz - 1, z + step, 1)]

    def from_z(k, step):
        for condition, at, way in sides(step):
            block = at * 2 + x
            take(condition, k, block, mine, z_up, up)
            if step < nz - 1:
                onward = jnp.logical_and(condition, z < nz - 1 if way == 0 else z > 0)
                send(onward, k, block, mine, (z_up, z_down)[way], (up, down)[way])
            send(condition, k, block, mine, over_x_sems, over_x)
            if step >= 2:
                send(condition, k, block, mine, over_y_sems, over_y)
            send(condition, k, block, mine, core_mine, over_c)

    def from_x(k, step):
        for condition, at, way in sides(step):
            block = at * 2 + 1 - x
            take(condition, k, block, mine, over_x_sems, over_x)
            if step >= 1:
                send(condition, k, block, mine, over_y_sems, over_y)
            send(condition, k, block, mine, core_mine, over_c)

    def from_y(k, step, column):
        for condition, at, way in sides(step):
            block = at * 2 + column
            take(condition, k, block, beside, over_y_sems, over_y)
            send(condition, k, block, beside, core_beside, over_c)

    def late(k):
        send(z < nz - 1, k, own, beside, z_up_late, up)
        send(z > 0, k, own, beside, z_down_late, down)
        send(None, k, own, beside, over_x_late, over_x)

    def from_late(k):
        take(None, k, z * 2 + 1 - x, beside, over_x_late, over_x)
        send(None, k, z * 2 + 1 - x, beside, core_beside, over_c)
        for condition, at, way in sides(1):
            take(condition, k, at * 2 + x, beside, z_up_late, up)
            send(condition, k, at * 2 + x, beside, core_beside, over_c)

    defer = max(nz - 2, 0)
    for step in range(nz + 2):
        for k in range(2):
            if 1 <= step < nz:
                from_z(k, step)
            if step == defer:
                late(k)
            if 0 <= step - 1 < nz:
                from_x(k, step - 1)
            if 2 <= step - 1 < nz:
                from_y(k, step - 1, x)
            if 1 <= step - 2 < nz:
                from_y(k, step - 2, 1 - x)
    for k in range(2):
        from_late(k)
    for k in range(2):
        for step in range(nz):
            for condition, at, way in sides(step):
                for column in (x, 1 - x):
                    if step >= 1 or column is not x:
                        block = at * 2 + column
                        take(condition, k, block, mine_other, core_mine, over_c)
                        take(condition, k, block, beside_other, core_beside, over_c)
    for k in range(1, count):
        source = (sp + count - k) % count
        remote(w_ref, ow_ref.at[source], w_sem.at[0, k], w_sem.at[1, k], over_x).wait_recv()
    for k in range(1, count):
        remote(w_ref, ow_ref.at[sp], w_sem.at[0, k], w_sem.at[1, k], over_x).wait_send()
    for condition, what in sends:
        guarded(condition, lambda: piece(*what).wait_send())
    for copy in locals_:
        copy.wait()


def gather_rows(nz, first, second, weights):
    count = 2 * nz
    rows, width = first.shape
    dma = pltpu.SemaphoreType.DMA
    whole = jax.ShapeDtypeStruct((count * rows, width), first.dtype)
    return pl.pallas_call(
        functools.partial(gather_kernel, nz),
        out_shape=(whole, whole, jax.ShapeDtypeStruct((count,) + weights.shape, weights.dtype)),
        in_specs=[pl.BlockSpec(memory_space=pltpu.VMEM)] * 3,
        out_specs=(pl.BlockSpec(memory_space=pl.ANY),) * 3,
        scratch_shapes=[
            dma((3,)),
            dma((4, 2, count)),
            dma((2, 2, count)),
            dma((4, 2, count)),
            dma((2, 2, count)),
            dma((2, 2, count)),
            dma((2, 2, count)),
            dma((2, count)),
        ],
        compiler_params=pltpu.CompilerParams(collective_id=0, has_side_effects=True),
        name="gather_rows",
    )(first, second, weights)


def total_kernel(
    nz, p_ref, o_ref, rc, s1, ra, rb, sa, sb, r2, s3, rz, full, c_sem, m_sem, n_sem, z_sem, g_sem
):
    width = p_ref.shape[1]
    half, quarter = width // 2, width // 4
    rows = p_ref.shape[0] // (2 * nz)
    sp, tp = lax.axis_index("sp"), lax.axis_index("tp")
    z, x, y, c = sp // 2, sp % 2, tp // 2, tp % 2
    over_x = (z * 2 + 1 - x, tp)
    over_y = (sp, (1 - y) * 2 + c)
    over_c = (sp, y * 2 + 1 - c)
    f32, bf16 = jnp.float32, jnp.bfloat16
    greet([(((z + k) % nz) * 2 + x, tp) for k in range(1, nz)] + [over_x, over_y, over_c])

    def lanes(index, size):
        return pl.ds(pl.multiple_of(index * size, size), size)

    def plane(i):
        return (z + 1 + i) % nz

    made = []

    def core_copy(i):
        at = lanes(plane(i), 2 * rows)
        return remote(
            p_ref.at[at, lanes(1 - c, half)], rc.at[at], c_sem.at[0, i], c_sem.at[1, i], over_c
        )

    for i in range(nz):
        copy = core_copy(i)
        copy.start()
        made.append(copy)
    firsts, seconds = [], []
    for i in range(nz):
        made[i].wait_recv()
        at = lanes(plane(i), 2 * rows)
        s1[at] = (p_ref[at, lanes(c, half)].astype(f32) + rc[at].astype(f32)).astype(bf16)
        if i % 2 == 0:
            copy = remote(
                s1.at[at, lanes(1 - y, quarter)],
                ra.at[i // 2],
                m_sem.at[0, i],
                m_sem.at[1, i],
                over_y,
            )
        else:
            copy = remote(
                s1.at[lanes(plane(i) * 2 + 1 - x, rows)],
                rb.at[i // 2],
                m_sem.at[0, i],
                m_sem.at[1, i],
                over_x,
            )
        copy.start()
        firsts.append(copy)
    for i in range(nz):
        firsts[i].wait_recv()
        k = i // 2
        if i % 2 == 0:
            at = lanes(plane(i), 2 * rows)
            sa[k] = (s1[at, lanes(y, quarter)].astype(f32) + ra[k].astype(f32)).astype(bf16)
            copy = remote(
                sa.at[k, lanes(1 - x, rows)], r2.at[i], n_sem.at[0, i], n_sem.at[1, i], over_x
            )
        else:
            at = lanes(plane(i) * 2 + x, rows)
            sb[k] = (s1[at].astype(f32) + rb[k].astype(f32)).astype(bf16)
            copy = remote(
                sb.at[k, :, lanes(1 - y, quarter)],
                r2.at[i],
                n_sem.at[0, i],
                n_sem.at[1, i],
                over_y,
            )
        copy.start()
        seconds.append(copy)
    along = []
    total = None
    for i in range(nz):
        seconds[i].wait_recv()
        k = i // 2
        held = sa[k, lanes(x, rows)] if i % 2 == 0 else sb[k, :, lanes(y, quarter)]
        value = held.astype(f32) + r2[i].astype(f32)
        if i < nz - 1:
            s3[i] = value.astype(bf16)
            copy = remote(
                s3.at[i], rz.at[i], z_sem.at[0, i], z_sem.at[1, i], (plane(i) * 2 + x, tp)
            )
            copy.start()
            along.append(copy)
        else:
            total = value
    for i in range(nz - 1):
        along[i].wait_recv()
        total = total + rz[i].astype(f32)
    mine = c * 2 + y
    theirs = c * 2 + 1 - y
    full[:, lanes(mine, quarter)] = total.astype(bf16)
    own = full.at[:, lanes(mine, quarter)]
    to_y = remote(own, own, g_sem.at[0, 0], g_sem.at[1, 0], over_y)
    to_c = remote(own, own, g_sem.at[0, 1], g_sem.at[1, 1], over_c)
    to_y.start()
    to_c.start()
    to_y.wait_recv()
    got = full.at[:, lanes(theirs, quarter)]
    onward = remote(got, got, g_sem.at[0, 2], g_sem.at[1, 2], over_c)
    onward.start()
    to_c.wait_recv()
    onward.wait_recv()
    o_ref[...] = full[...]
    for copy in made + firsts + seconds + along + [to_y, to_c, onward]:
        copy.wait_send()


def total_rows(nz, parts):
    count = 2 * nz
    rows, width = parts.shape[0] // count, parts.shape[1]
    half, quarter = width // 2, width // 4
    evens, odds = (nz + 1) // 2, max(nz // 2, 1)
    dma = pltpu.SemaphoreType.DMA
    vmem = functools.partial(pltpu.VMEM, dtype=jnp.bfloat16)
    return pl.pallas_call(
        functools.partial(total_kernel, nz),
        out_shape=jax.ShapeDtypeStruct((rows, width), jnp.bfloat16),
        in_specs=[pl.BlockSpec(memory_space=pltpu.VMEM)],
        out_specs=pl.BlockSpec(memory_space=pltpu.VMEM),
        scratch_shapes=[
            vmem((count * rows, half)),
            vmem((count * rows, half)),
            vmem((evens, 2 * rows, quarter)),
            vmem((odds, rows, half)),
            vmem((evens, 2 * rows, quarter)),
            vmem((odds, rows, half)),
            vmem((nz, rows, quarter)),
            vmem((nz, rows, quarter)),
            vmem((nz, rows, quarter)),
            vmem((rows, width)),
            dma((2, nz)),
            dma((2, nz)),
            dma((2, nz)),
            dma((2, nz)),
            dma((2, 3)),
        ],
        compiler_params=pltpu.CompilerParams(collective_id=1, has_side_effects=True),
        name="total_rows",
    )(parts)


def carry_kernel(
    nz, coef_ref, carry_ref, p_ref, later_ref, o_ref, rc, px, sx, pz, r_sem, x_sem, z_sem
):
    count = 2 * nz
    rows = p_ref.shape[0] // count
    heads = coef_ref.shape[1]
    per_head = carry_ref.shape[0] // heads
    sp, tp = lax.axis_index("sp"), lax.axis_index("tp")
    z, x = sp // 2, sp % 2
    over_x = (z * 2 + 1 - x, tp)
    f32, bf16 = jnp.float32, jnp.bfloat16
    greet([((sp + k) % count, tp) for k in range(1, count)])

    def block(index):
        return pl.ds(pl.multiple_of(index * rows, rows), rows)

    def plane(i):
        return (z + 1 + i) % nz

    firsts, along = [], []
    for i in range(nz):
        copy = remote(
            p_ref.at[block(plane(i) * 2 + 1 - x)],
            px.at[i],
            x_sem.at[0, i],
            x_sem.at[1, i],
            over_x,
        )
        copy.start()
        firsts.append(copy)

    def carry_copy(d):
        target = (jnp.maximum(sp - d, 0), tp)
        return remote(carry_ref, rc.at[d], r_sem.at[0, d], r_sem.at[1, d], target)

    for d in range(1, count):
        pl.when(sp - d >= 0)(lambda: carry_copy(d).start())
    total = None
    for i in range(nz):
        firsts[i].wait_recv()
        value = p_ref[block(plane(i) * 2 + x)].astype(f32) + px[i].astype(f32)
        if i < nz - 1:
            sx[i] = value.astype(bf16)
            copy = remote(
                sx.at[i], pz.at[i], z_sem.at[0, i], z_sem.at[1, i], (plane(i) * 2 + x, tp)
            )
            copy.start()
            along.append(copy)
        else:
            o_ref[...] = value
    later_ref[...] = jnp.zeros_like(later_ref)
    for d in range(1, count):

        @pl.when(sp + d < count)
        def _():
            carry_copy(d).wait_recv()
            for h in range(heads):
                at = pl.ds(h * per_head, per_head)
                later_ref[at] += coef_ref[d - 1, h] * rc[d, at].astype(f32)

    for i in range(nz - 1):
        along[i].wait_recv()
        o_ref[...] += pz[i].astype(f32)
    for copy in firsts + along:
        copy.wait_send()
    for d in range(1, count):
        pl.when(sp - d >= 0)(lambda: carry_copy(d).wait_send())


def carry_and_total(nz, decays, carried, parts):
    count = 2 * nz
    heads, channels, states = carried.shape
    lanes = 128
    place = lax.axis_index("sp")
    padded = jnp.concatenate([decays, jnp.ones_like(decays)])
    ahead = lax.dynamic_slice_in_dim(padded, place + 1, count - 1, 0)
    coefs = jnp.concatenate([jnp.ones_like(ahead[:1]), jnp.cumprod(ahead[:-1], axis=0)])
    flat = carried.astype(jnp.bfloat16).reshape(-1, lanes)
    rows, width = parts.shape[0] // count, parts.shape[1]
    dma = pltpu.SemaphoreType.DMA
    vmem = functools.partial(pltpu.VMEM, dtype=jnp.bfloat16)
    space = pl.BlockSpec(memory_space=pltpu.VMEM)
    later, total = pl.pallas_call(
        functools.partial(carry_kernel, nz),
        out_shape=(
            jax.ShapeDtypeStruct(flat.shape, jnp.float32),
            jax.ShapeDtypeStruct((rows, width), jnp.float32),
        ),
        in_specs=[pl.BlockSpec(memory_space=pltpu.SMEM), space, space],
        out_specs=(space, space),
        scratch_shapes=[
            vmem((count,) + flat.shape),
            vmem((nz, rows, width)),
            vmem((nz, rows, width)),
            vmem((nz, rows, width)),
            dma((2, count)),
            dma((2, nz)),
            dma((2, nz)),
        ],
        compiler_params=pltpu.CompilerParams(collective_id=2, has_side_effects=True),
        name="carry_and_total",
    )(coefs, flat, parts.astype(jnp.bfloat16))
    return later.reshape(heads, channels, states), total


def dense_grads(normed, cotangent, routes, route_weight, decay_now, gate_mat, up_mat, down_mat):
    sp_count = lax.axis_size("sp")
    experts_count = sp_count // 2
    nz = sp_count // 2
    names = jnp.arange(experts_count, dtype=jnp.int32)[:, None]
    table = jnp.where(routes[None, :, 0] == names, route_weight[None, :, 0], 0.0)
    table = table + jnp.where(routes[None, :, 1] == names, route_weight[None, :, 1], 0.0)
    spread = jnp.broadcast_to(decay_now[:, None], (decay_now.shape[0], table.shape[1]))
    table = jnp.concatenate([table, spread])
    rows_in, cot_all, tables = gather_rows(nz, normed, cotangent, table)
    decays = tables[:, experts_count:, 0]
    weight_all = lax.dynamic_index_in_dim(tables, lax.axis_index("sp") // 2, 1, False).reshape(-1)
    rows_cot = (weight_all[:, None] * cot_all.astype(jnp.float32)).astype(jnp.bfloat16)
    gate_grad, up_grad, down_grad, input_part = expert_grads(
        rows_in, rows_cot, gate_mat, up_mat, down_mat
    )
    normed_grad = total_rows(nz, input_part.astype(jnp.bfloat16)).astype(jnp.float32)
    return gate_grad, up_grad, down_grad, normed_grad, decays


def routed_grads(normed, cotangent, routes, route_weight, gate_mat, up_mat, down_mat):
    sp_count = lax.axis_size("sp")
    tp_count = lax.axis_size("tp")
    tok_rows = normed.shape[0]
    experts_count = sp_count // 2
    capacity = min(tok_rows, 4 * tok_rows // experts_count)
    quarter = D // tp_count
    route_flat = routes.reshape(-1)
    member = (route_flat[:, None] == jnp.arange(experts_count, dtype=jnp.int32)[None, :]).astype(
        jnp.int32
    )
    earlier_count = jnp.sum((jnp.cumsum(member, axis=0) - member) * member, axis=1)
    places = (route_flat * capacity + earlier_count).reshape(tok_rows, 2)
    slot_ids = jnp.arange(experts_count * capacity, dtype=jnp.int32)[:, None]
    first_hit = slot_ids == places[None, :, 0]
    second_hit = slot_ids == places[None, :, 1]
    placing = jnp.logical_or(first_hit, second_hit)
    place_matrix = placing.astype(jnp.bfloat16)
    slot_weight = jnp.sum(
        jnp.where(first_hit, route_weight[None, :, 0], 0.0)
        + jnp.where(second_hit, route_weight[None, :, 1], 0.0),
        axis=1,
    )
    send_in = jnp.dot(place_matrix, normed, preferred_element_type=jnp.float32).astype(jnp.bfloat16)
    send_cot = (
        slot_weight[:, None] * jnp.dot(place_matrix, cotangent, preferred_element_type=jnp.float32)
    ).astype(jnp.bfloat16)
    half_cap = capacity // 2
    part_in, part_cot = (
        lax.all_to_all(
            send_in.reshape(sp_count, half_cap, D), "sp", split_axis=0, concat_axis=0, tiled=True
        ),
        lax.all_to_all(
            send_cot.reshape(sp_count, half_cap, D), "sp", split_axis=0, concat_axis=0, tiled=True
        ),
    )
    other_in, other_cot = swapped((part_in, part_cot), "sp", 0)
    lower_bit = lax.axis_index("sp") % 2 == 0
    recv_in = jnp.concatenate(
        [jnp.where(lower_bit, part_in, other_in), jnp.where(lower_bit, other_in, part_in)], axis=1
    )
    recv_cot = jnp.concatenate(
        [jnp.where(lower_bit, part_cot, other_cot), jnp.where(lower_bit, other_cot, part_cot)],
        axis=1,
    )
    rows_in = recv_in.reshape(-1, D)
    rows_cot = recv_cot.reshape(-1, D)
    gate_grad, up_grad, down_grad, input_part = expert_grads(
        rows_in, rows_cot, gate_mat, up_mat, down_mat
    )
    input_quarter = lax.psum_scatter(input_part, "tp", scatter_dimension=1, tiled=True)
    returned = lax.all_to_all(
        input_quarter.reshape(sp_count, capacity, quarter),
        "sp",
        split_axis=0,
        concat_axis=0,
        tiled=True,
    )
    pair_total = jnp.sum(returned.reshape(experts_count, 2, capacity, quarter), axis=1).reshape(
        -1, quarter
    )
    token_quarter = lax.dot_general(
        placing.astype(jnp.float32), pair_total, (((0,), (0,)), ((), ())), precision=HIGHEST
    )
    normed_grad = lax.all_gather(token_quarter, "tp", axis=1, tiled=True)
    return gate_grad, up_grad, down_grad, normed_grad


def shards(
    tokens,
    norm_gain,
    cotangent,
    routes,
    route_weight,
    gate_weight,
    up_weight,
    down_weight,
    scan_input,
    out_gate,
    step_size,
    decay_rate,
    write_keys,
    read_keys,
    start_state,
    out_proj,
):
    sp_count = lax.axis_size("sp")
    tp_count = lax.axis_size("tp")
    tok_rows = tokens.shape[0]
    experts_count = sp_count // 2
    capacity = min(tok_rows, 4 * tok_rows // experts_count)
    quarter = D // tp_count
    hidden = tokens.astype(jnp.float32)
    inverse = lax.rsqrt(jnp.mean(hidden * hidden, axis=1) + EPS)
    normed = (hidden * inverse[:, None] * norm_gain[None, :]).astype(jnp.bfloat16)
    dense = capacity == tok_rows and tp_count == 4
    mats = (gate_weight[0], up_weight[0], down_weight[0])
    if dense:
        decay_now = jnp.exp(jnp.sum(-decay_rate[:, None] * step_size, axis=1))
        gate_grad, up_grad, down_grad, normed_grad, decays = dense_grads(
            normed, cotangent, routes, route_weight, decay_now, *mats
        )
    else:
        gate_grad, up_grad, down_grad, normed_grad = routed_grads(
            normed, cotangent, routes, route_weight, *mats
        )
    gained = norm_gain[None, :] * normed_grad
    dotted = jnp.sum(hidden * gained, axis=1)
    residual = (
        cotangent.astype(jnp.float32)
        + inverse[:, None] * gained
        - hidden * (inverse**3 * dotted / D)[:, None]
    )
    residual_grad = residual.astype(jnp.bfloat16)
    mix_grad = jnp.dot(residual_grad, out_proj, preferred_element_type=jnp.float32)
    per_group = HEADS // GROUPS
    gated, gate_out_grad, decay_now, carried, state_grad = block_forward(
        scan_input,
        out_gate,
        step_size,
        write_keys,
        read_keys,
        decay_rate,
        start_state[0],
        mix_grad,
        per_group,
    )
    proj_part = lax.dot_general(
        residual_grad, gated, (((0,), (0,)), ((), ())), preferred_element_type=jnp.float32
    )
    if dense:
        later_state, out_proj_grad = carry_and_total(sp_count // 2, decays, carried, proj_part)
    else:
        totals, later_state = prefix(
            (decay_now, carried), "sp", compose, (jnp.ones_like(decay_now), jnp.zeros_like(carried))
        )
        out_proj_grad = lax.psum_scatter(proj_part, "sp", scatter_dimension=0, tiled=True)
    scan_grad, write_grad, read_grad = block_back(
        scan_input,
        step_size,
        write_keys,
        read_keys,
        decay_rate,
        start_state[0],
        state_grad,
        later_state,
        per_group,
    )
    residual_part = lax.dynamic_slice_in_dim(
        residual_grad, lax.axis_index("tp") * quarter, quarter, 1
    )
    return (
        residual_part,
        gate_grad.astype(jnp.bfloat16)[None],
        up_grad.astype(jnp.bfloat16)[None],
        down_grad.astype(jnp.bfloat16)[None],
        out_proj_grad,
        scan_grad,
        gate_out_grad,
        write_grad,
        read_grad,
    )


def solution(mesh):
    return jax.shard_map(
        shards,
        mesh=mesh,
        in_specs=(
            P("sp", None),
            P(),
            P("sp", None),
            P("sp", None),
            P("sp", None),
            P("sp", None, "tp"),
            P("sp", None, "tp"),
            P("sp", "tp", None),
            P("sp", "tp"),
            P("sp", "tp"),
            P("tp", "sp"),
            P("tp"),
            P("sp", "tp"),
            P("sp", "tp"),
            P("sp", "tp", None, None),
            P(None, "tp"),
        ),
        out_specs=(
            P("sp", "tp"),
            P("sp", None, "tp"),
            P("sp", None, "tp"),
            P("sp", "tp", None),
            P("sp", "tp"),
            P("sp", "tp"),
            P("sp", "tp"),
            P("sp", "tp"),
            P("sp", "tp"),
        ),
        check_vma=False,
    )
```

```python
import functools

import jax
import jax.numpy as jnp
from jax import lax
from jax.experimental import pallas as pl
from jax.experimental.pallas import tpu as pltpu
from jax.sharding import PartitionSpec as P

D = 2048
HEADS = 16
STATE = 64
GROUPS = 4


EPS = 1e-06
HIGHEST = lax.Precision.HIGHEST


def swapped(value, axis, apart):
    mask = 2**apart
    pairs = [(source, source ^ mask) for source in range(lax.axis_size(axis))]
    return lax.ppermute(value, axis, pairs)


def prefix(part, axis, combine, identity):
    count = lax.axis_size(axis)
    place = lax.axis_index(axis)
    ahead = count - 1 - place
    gathered = jax.tree.map(lambda a: lax.all_gather(a, axis), part)
    state = jax.tree.map(lambda a, e: jnp.zeros_like(a) + jnp.asarray(e, a.dtype), part, identity)

    def one(hop, state):
        source = count - 1 - hop
        return combine(
            state, jax.tree.map(lambda a: lax.dynamic_index_in_dim(a, source, 0, False), gathered)
        )

    return lax.fori_loop(0, ahead, one, state)


def prepare(scan_rows, step_rows, write_rows, read_rows, decay_rates, per_group):
    length = scan_rows.shape[0]
    head_count = step_rows.shape[0]
    logdec = jnp.cumsum(-decay_rates[:, None] * step_rows, axis=1)
    causal = jnp.arange(length)[:, None] >= jnp.arange(length)[None, :]
    spread = jnp.where(causal[None, :, :], logdec[:, :, None] - logdec[:, None, :], -jnp.inf)
    weights = jnp.exp(spread)
    inputs = (
        scan_rows.astype(jnp.float32).reshape(length, head_count, -1)
        * jnp.transpose(step_rows)[:, :, None]
    )
    write_head = jnp.repeat(
        write_rows.astype(jnp.float32).reshape(length, -1, STATE), per_group, axis=1
    )
    read_head = jnp.repeat(
        read_rows.astype(jnp.float32).reshape(length, -1, STATE), per_group, axis=1
    )
    scores = jnp.einsum("thn,shn->hts", read_head, write_head, precision=HIGHEST) * weights
    return (logdec, weights, inputs, write_head, read_head, scores)


def block_forward(
    scan_rows,
    gate_rows,
    step_rows,
    write_rows,
    read_rows,
    decay_rates,
    entry_state,
    mix_grad,
    per_group,
):
    logdec, weights, inputs, write_head, read_head, scores = prepare(
        scan_rows, step_rows, write_rows, read_rows, decay_rates, per_group
    )
    length, head_count = (inputs.shape[0], inputs.shape[1])
    growth = jnp.transpose(jnp.exp(logdec))
    output = jnp.einsum("hts,shp->thp", scores, inputs, precision=HIGHEST)
    output = output + growth[:, :, None] * jnp.einsum(
        "thn,hpn->thp", read_head, entry_state, precision=HIGHEST
    )
    gate_val = gate_rows.astype(jnp.float32).reshape(length, head_count, -1)
    sigmoid_val = jax.nn.sigmoid(gate_val)
    gated = (output * gate_val * sigmoid_val).reshape(length, -1).astype(jnp.bfloat16)
    out_grad = mix_grad.reshape(length, head_count, -1)
    state_grad = out_grad * gate_val * sigmoid_val
    gate_grad = (
        (out_grad * output * sigmoid_val * (1.0 + gate_val * (1.0 - sigmoid_val)))
        .reshape(length, -1)
        .astype(jnp.bfloat16)
    )
    carried = jnp.einsum("th,thp,thn->hpn", growth, state_grad, read_head, precision=HIGHEST)
    return (gated, gate_grad, jnp.exp(logdec[:, -1]), carried, state_grad)


def block_back(
    scan_rows,
    step_rows,
    write_rows,
    read_rows,
    decay_rates,
    entry_state,
    state_grad,
    later_state,
    per_group,
):
    logdec, weights, inputs, write_head, read_head, scores = prepare(
        scan_rows, step_rows, write_rows, read_rows, decay_rates, per_group
    )
    length, head_count = (inputs.shape[0], inputs.shape[1])
    growth = jnp.transpose(jnp.exp(logdec))
    shrink = jnp.transpose(jnp.exp(logdec[:, -1:] - logdec))
    in_grad = jnp.einsum("hts,thp->shp", scores, state_grad, precision=HIGHEST)
    in_grad = in_grad + shrink[:, :, None] * jnp.einsum(
        "shn,hpn->shp", write_head, later_state, precision=HIGHEST
    )
    scan_grad = (
        (in_grad * jnp.transpose(step_rows)[:, :, None]).reshape(length, -1).astype(jnp.bfloat16)
    )
    pair_terms = jnp.einsum("thp,shp->hts", state_grad, inputs, precision=HIGHEST) * weights
    read_grad = jnp.einsum("hts,shn->thn", pair_terms, write_head, precision=HIGHEST)
    read_grad = read_grad + growth[:, :, None] * jnp.einsum(
        "thp,hpn->thn", state_grad, entry_state, precision=HIGHEST
    )
    write_grad = jnp.einsum("hts,thn->shn", pair_terms, read_head, precision=HIGHEST)
    write_grad = write_grad + shrink[:, :, None] * jnp.einsum(
        "shp,hpn->shn", inputs, later_state, precision=HIGHEST
    )
    group_count = head_count // per_group
    read_total = (
        jnp.sum(read_grad.reshape(length, group_count, per_group, -1), axis=2)
        .reshape(length, -1)
        .astype(jnp.bfloat16)
    )
    write_total = (
        jnp.sum(write_grad.reshape(length, group_count, per_group, -1), axis=2)
        .reshape(length, -1)
        .astype(jnp.bfloat16)
    )
    return (scan_grad, write_total, read_total)


def expert_grads(rows_in, rows_cot, gate_mat, up_mat, down_mat):
    contract_rows = (((0,), (0,)), ((), ()))
    contract_cols = (((1,), (1,)), ((), ()))
    gate_pre = jnp.dot(rows_in, gate_mat, preferred_element_type=jnp.float32)
    up_pre = jnp.dot(rows_in, up_mat, preferred_element_type=jnp.float32)
    sigmoid_val = jax.nn.sigmoid(gate_pre)
    active = (gate_pre * sigmoid_val * up_pre).astype(jnp.bfloat16)
    down_grad = lax.dot_general(active, rows_cot, contract_rows, preferred_element_type=jnp.float32)
    act_grad = lax.dot_general(
        rows_cot, down_mat, contract_cols, preferred_element_type=jnp.float32
    )
    gate_pre_grad = (
        act_grad * up_pre * sigmoid_val * (1.0 + gate_pre * (1.0 - sigmoid_val))
    ).astype(jnp.bfloat16)
    up_pre_grad = (act_grad * gate_pre * sigmoid_val).astype(jnp.bfloat16)
    gate_grad = lax.dot_general(
        rows_in, gate_pre_grad, contract_rows, preferred_element_type=jnp.float32
    )
    up_grad = lax.dot_general(
        rows_in, up_pre_grad, contract_rows, preferred_element_type=jnp.float32
    )
    input_grad = lax.dot_general(
        gate_pre_grad, gate_mat, contract_cols, preferred_element_type=jnp.float32
    )
    input_grad = input_grad + lax.dot_general(
        up_pre_grad, up_mat, contract_cols, preferred_element_type=jnp.float32
    )
    return (gate_grad, up_grad, down_grad, input_grad)


def compose(higher, nearer):
    return (nearer[0] * higher[0], nearer[1] + nearer[0][:, None, None] * higher[1])


MESH = pl.DeviceIdType.MESH


def remote(src, dst, send, recv, device):
    return pltpu.make_async_remote_copy(
        src_ref=src,
        dst_ref=dst,
        send_sem=send,
        recv_sem=recv,
        device_id=device,
        device_id_type=MESH,
    )


def greet(devices):
    barrier = pltpu.get_barrier_semaphore()
    for device in devices:
        pl.semaphore_signal(barrier, inc=1, device_id=device, device_id_type=MESH)
    pl.semaphore_wait(barrier, len(devices))


def gather_kernel(
    nz,
    a_ref,
    b_ref,
    w_ref,
    oa_ref,
    ob_ref,
    ow_ref,
    own_sem,
    z_send,
    z_recv,
    x_sem,
    y_sem,
    c_sem,
    d_sem,
    w_sem,
):
    rows = a_ref.shape[0]
    part = rows // 4
    sp, tp = lax.axis_index("sp"), lax.axis_index("tp")
    z, x, y, c = sp // 2, sp % 2, tp // 2, tp % 2
    count = 2 * nz
    over_x = (z * 2 + 1 - x, tp)
    over_y = (sp, (1 - y) * 2 + c)
    over_c = (sp, y * 2 + 1 - c)
    peers = [((sp + k) % count, tp) for k in range(1, count)]
    greet(peers + [over_y, over_c])

    mine = (c * 2 + y) * part
    beside = (c * 2 + 1 - y) * part
    mine_other = ((1 - c) * 2 + y) * part
    beside_other = ((1 - c) * 2 + 1 - y) * part
    pairs = ((a_ref, oa_ref), (b_ref, ob_ref))
    own = z * 2 + x
    up = (jnp.minimum(z + 1, nz - 1) * 2 + x, tp)
    down = (jnp.maximum(z - 1, 0) * 2 + x, tp)
    sends = []

    def piece(k, block, start, sems, device):
        src, dst = pairs[k]
        at = dst.at[pl.ds(pl.multiple_of(block * rows + start, part), part)]
        source = at
        if block is own:
            source = src.at[pl.ds(pl.multiple_of(start, part), part)]
        return remote(source, at, sems[0].at[k, block], sems[1].at[k, block], device)

    def guarded(condition, work):
        if condition is None:
            work()
        else:
            pl.when(condition)(work)

    def send(condition, *what):
        guarded(condition, lambda: piece(*what).start())
        sends.append((condition, what))

    def take(condition, *what):
        guarded(condition, lambda: piece(*what).wait_recv())

    z_up, z_down = (z_send.at[0], z_recv.at[0]), (z_send.at[1], z_recv.at[0])
    z_up_late, z_down_late = (z_send.at[2], z_recv.at[1]), (z_send.at[3], z_recv.at[1])
    over_x_sems, over_x_late = (x_sem.at[0], x_sem.at[1]), (x_sem.at[2], x_sem.at[3])
    over_y_sems = (y_sem.at[0], y_sem.at[1])
    core_mine, core_beside = (c_sem.at[0], c_sem.at[1]), (d_sem.at[0], d_sem.at[1])
    for k in range(2):
        send(z < nz - 1, k, own, mine, z_up, up)
        send(z > 0, k, own, mine, z_down, down)
        send(None, k, own, mine, over_x_sems, over_x)
    for k in range(1, count):
        other = ((sp + k) % count, tp)
        remote(w_ref, ow_ref.at[sp], w_sem.at[0, k], w_sem.at[1, k], other).start()
    locals_ = [
        pltpu.make_async_copy(src, dst.at[pl.ds(pl.multiple_of(own * rows, rows), rows)], own_sem.at[k])
        for k, (src, dst) in enumerate(pairs)
    ]
    locals_.append(pltpu.make_async_copy(w_ref, ow_ref.at[sp], own_sem.at[2]))
    for copy in locals_:
        copy.start()

    def sides(step):
        if step == 0:
            return [(None, z, 0)]
        return [(z - step >= 0, z - step, 0), (z + step <= nz - 1, z + step, 1)]

    def from_z(k, step):
        for condition, at, way in sides(step):
            block = at * 2 + x
            take(condition, k, block, mine, z_up, up)
            if step < nz - 1:
                onward = jnp.logical_and(condition, z < nz - 1 if way == 0 else z > 0)
                send(onward, k, block, mine, (z_up, z_down)[way], (up, down)[way])
            send(condition, k, block, mine, over_x_sems, over_x)
            if step >= 2:
                send(condition, k, block, mine, over_y_sems, over_y)
            send(condition, k, block, mine, core_mine, over_c)

    def from_x(k, step):
        for condition, at, way in sides(step):
            block = at * 2 + 1 - x
            take(condition, k, block, mine, over_x_sems, over_x)
            if step >= 1:
                send(condition, k, block, mine, over_y_sems, over_y)
            send(condition, k, block, mine, core_mine, over_c)

    def from_y(k, step, column):
        for condition, at, way in sides(step):
            block = at * 2 + column
            take(condition, k, block, beside, over_y_sems, over_y)
            send(condition, k, block, beside, core_beside, over_c)

    def late(k):
        send(z < nz - 1, k, own, beside, z_up_late, up)
        send(z > 0, k, own, beside, z_down_late, down)
        send(None, k, own, beside, over_x_late, over_x)

    def from_late(k):
        take(None, k, z * 2 + 1 - x, beside, over_x_late, over_x)
        send(None, k, z * 2 + 1 - x, beside, core_beside, over_c)
        for condition, at, way in sides(1):
            take(condition, k, at * 2 + x, beside, z_up_late, up)
            send(condition, k, at * 2 + x, beside, core_beside, over_c)

    defer = max(nz - 2, 0)
    for step in range(nz + 2):
        for k in range(2):
            if 1 <= step < nz:
                from_z(k, step)
            if step == defer:
                late(k)
            if 0 <= step - 1 < nz:
                from_x(k, step - 1)
            if 2 <= step - 1 < nz:
                from_y(k, step - 1, x)
            if 1 <= step - 2 < nz:
                from_y(k, step - 2, 1 - x)
    for k in range(2):
        from_late(k)
    for k in range(2):
        for step in range(nz):
            for condition, at, way in sides(step):
                for column in (x, 1 - x):
                    if step >= 1 or column is not x:
                        block = at * 2 + column
                        take(condition, k, block, mine_other, core_mine, over_c)
                        take(condition, k, block, beside_other, core_beside, over_c)
    for k in range(1, count):
        source = (sp + count - k) % count
        remote(w_ref, ow_ref.at[source], w_sem.at[0, k], w_sem.at[1, k], over_x).wait_recv()
    for k in range(1, count):
        remote(w_ref, ow_ref.at[sp], w_sem.at[0, k], w_sem.at[1, k], over_x).wait_send()
    for condition, what in sends:
        guarded(condition, lambda: piece(*what).wait_send())
    for copy in locals_:
        copy.wait()


def gather_rows(nz, first, second, weights):
    count = 2 * nz
    rows, width = first.shape
    dma = pltpu.SemaphoreType.DMA
    whole = jax.ShapeDtypeStruct((count * rows, width), first.dtype)
    return pl.pallas_call(
        functools.partial(gather_kernel, nz),
        out_shape=(whole, whole, jax.ShapeDtypeStruct((count,) + weights.shape, weights.dtype)),
        in_specs=[pl.BlockSpec(memory_space=pltpu.VMEM)] * 3,
        out_specs=(pl.BlockSpec(memory_space=pl.ANY),) * 3,
        scratch_shapes=[
            dma((3,)),
            dma((4, 2, count)),
            dma((2, 2, count)),
            dma((4, 2, count)),
            dma((2, 2, count)),
            dma((2, 2, count)),
            dma((2, 2, count)),
            dma((2, count)),
        ],
        compiler_params=pltpu.CompilerParams(collective_id=0, has_side_effects=True),
        name="gather_rows",
    )(first, second, weights)


def total_kernel(
    nz, p_ref, o_ref, rc, s1, ra, rb, sa, sb, r2, s3, rz, full, c_sem, m_sem, n_sem, z_sem, g_sem
):
    width = p_ref.shape[1]
    half, quarter = width // 2, width // 4
    rows = p_ref.shape[0] // (2 * nz)
    sp, tp = lax.axis_index("sp"), lax.axis_index("tp")
    z, x, y, c = sp // 2, sp % 2, tp // 2, tp % 2
    over_x = (z * 2 + 1 - x, tp)
    over_y = (sp, (1 - y) * 2 + c)
    over_c = (sp, y * 2 + 1 - c)
    f32, bf16 = jnp.float32, jnp.bfloat16
    greet([(((z + k) % nz) * 2 + x, tp) for k in range(1, nz)] + [over_x, over_y, over_c])

    def lanes(index, size):
        return pl.ds(pl.multiple_of(index * size, size), size)

    def plane(i):
        return (z + 1 + i) % nz

    made = []

    def core_copy(i):
        at = lanes(plane(i), 2 * rows)
        return remote(
            p_ref.at[at, lanes(1 - c, half)], rc.at[at], c_sem.at[0, i], c_sem.at[1, i], over_c
        )

    for i in range(nz):
        copy = core_copy(i)
        copy.start()
        made.append(copy)
    firsts, seconds, along = [], [], []

    def first(i):
        made[i].wait_recv()
        at = lanes(plane(i), 2 * rows)
        s1[at] = (p_ref[at, lanes(c, half)].astype(f32) + rc[at].astype(f32)).astype(bf16)
        sems = (m_sem.at[0, i], m_sem.at[1, i])
        if i % 2 == 0:
            copy = remote(s1.at[at, lanes(1 - y, quarter)], ra.at[i // 2], *sems, over_y)
        else:
            block = lanes(plane(i) * 2 + 1 - x, rows)
            copy = remote(s1.at[block], rb.at[i // 2], *sems, over_x)
        copy.start()
        firsts.append(copy)

    def second(i):
        firsts[i].wait_recv()
        k = i // 2
        sems = (n_sem.at[0, i], n_sem.at[1, i])
        if i % 2 == 0:
            at = lanes(plane(i), 2 * rows)
            sa[k] = (s1[at, lanes(y, quarter)].astype(f32) + ra[k].astype(f32)).astype(bf16)
            copy = remote(sa.at[k, lanes(1 - x, rows)], r2.at[i], *sems, over_x)
        else:
            at = lanes(plane(i) * 2 + x, rows)
            sb[k] = (s1[at].astype(f32) + rb[k].astype(f32)).astype(bf16)
            copy = remote(sb.at[k, :, lanes(1 - y, quarter)], r2.at[i], *sems, over_y)
        copy.start()
        seconds.append(copy)

    def third(i):
        seconds[i].wait_recv()
        k = i // 2
        held = sa[k, lanes(x, rows)] if i % 2 == 0 else sb[k, :, lanes(y, quarter)]
        value = held.astype(f32) + r2[i].astype(f32)
        if i < nz - 1:
            s3[i] = value.astype(bf16)
            target = (plane(i) * 2 + x, tp)
            copy = remote(s3.at[i], rz.at[i], z_sem.at[0, i], z_sem.at[1, i], target)
            copy.start()
            along.append(copy)
        return value

    lead = min(3, nz)
    for i in range(lead):
        first(i)
    for i in range(nz):
        second(i)
        if i + lead < nz:
            first(i + lead)
        if i > 0:
            third(i - 1)
    total = third(nz - 1)
    for i in range(nz - 1):
        along[i].wait_recv()
        total = total + rz[i].astype(f32)
    mine = c * 2 + y
    theirs = c * 2 + 1 - y
    full[:, lanes(mine, quarter)] = total.astype(bf16)
    own = full.at[:, lanes(mine, quarter)]
    to_y = remote(own, own, g_sem.at[0, 0], g_sem.at[1, 0], over_y)
    to_c = remote(own, own, g_sem.at[0, 1], g_sem.at[1, 1], over_c)
    to_y.start()
    to_c.start()
    to_y.wait_recv()
    got = full.at[:, lanes(theirs, quarter)]
    onward = remote(got, got, g_sem.at[0, 2], g_sem.at[1, 2], over_c)
    onward.start()
    to_c.wait_recv()
    onward.wait_recv()
    o_ref[...] = full[...]
    for copy in made + firsts + seconds + along + [to_y, to_c, onward]:
        copy.wait_send()


def total_rows(nz, parts):
    count = 2 * nz
    rows, width = parts.shape[0] // count, parts.shape[1]
    half, quarter = width // 2, width // 4
    evens, odds = (nz + 1) // 2, max(nz // 2, 1)
    dma = pltpu.SemaphoreType.DMA
    vmem = functools.partial(pltpu.VMEM, dtype=jnp.bfloat16)
    return pl.pallas_call(
        functools.partial(total_kernel, nz),
        out_shape=jax.ShapeDtypeStruct((rows, width), jnp.bfloat16),
        in_specs=[pl.BlockSpec(memory_space=pltpu.VMEM)],
        out_specs=pl.BlockSpec(memory_space=pltpu.VMEM),
        scratch_shapes=[
            vmem((count * rows, half)),
            vmem((count * rows, half)),
            vmem((evens, 2 * rows, quarter)),
            vmem((odds, rows, half)),
            vmem((evens, 2 * rows, quarter)),
            vmem((odds, rows, half)),
            vmem((nz, rows, quarter)),
            vmem((nz, rows, quarter)),
            vmem((nz, rows, quarter)),
            vmem((rows, width)),
            dma((2, nz)),
            dma((2, nz)),
            dma((2, nz)),
            dma((2, nz)),
            dma((2, 3)),
        ],
        compiler_params=pltpu.CompilerParams(collective_id=1, has_side_effects=True),
        name="total_rows",
    )(parts)


def carry_kernel(
    nz, coef_ref, carry_ref, p_ref, later_ref, o_ref, rc, px, sx, pz, r_sem, x_sem, z_sem
):
    count = 2 * nz
    rows = p_ref.shape[0] // count
    heads = coef_ref.shape[1]
    per_head = carry_ref.shape[0] // heads
    sp, tp = lax.axis_index("sp"), lax.axis_index("tp")
    z, x = sp // 2, sp % 2
    over_x = (z * 2 + 1 - x, tp)
    f32, bf16 = jnp.float32, jnp.bfloat16
    greet([((sp + k) % count, tp) for k in range(1, count)])

    def block(index):
        return pl.ds(pl.multiple_of(index * rows, rows), rows)

    def plane(i):
        return (z + 1 + i) % nz

    firsts, along = [], []
    for i in range(nz):
        copy = remote(
            p_ref.at[block(plane(i) * 2 + 1 - x)],
            px.at[i],
            x_sem.at[0, i],
            x_sem.at[1, i],
            over_x,
        )
        copy.start()
        firsts.append(copy)

    def carry_copy(d):
        target = (jnp.maximum(sp - d, 0), tp)
        return remote(carry_ref, rc.at[d], r_sem.at[0, d], r_sem.at[1, d], target)

    for d in range(1, count):
        pl.when(sp - d >= 0)(lambda: carry_copy(d).start())
    total = None
    for i in range(nz):
        firsts[i].wait_recv()
        value = p_ref[block(plane(i) * 2 + x)].astype(f32) + px[i].astype(f32)
        if i < nz - 1:
            sx[i] = value.astype(bf16)
            copy = remote(
                sx.at[i], pz.at[i], z_sem.at[0, i], z_sem.at[1, i], (plane(i) * 2 + x, tp)
            )
            copy.start()
            along.append(copy)
        else:
            o_ref[...] = value
    later_ref[...] = jnp.zeros_like(later_ref)
    for d in range(1, count):

        @pl.when(sp + d < count)
        def _():
            carry_copy(d).wait_recv()
            for h in range(heads):
                at = pl.ds(h * per_head, per_head)
                later_ref[at] += coef_ref[d - 1, h] * rc[d, at].astype(f32)

    for i in range(nz - 1):
        along[i].wait_recv()
        o_ref[...] += pz[i].astype(f32)
    for copy in firsts + along:
        copy.wait_send()
    for d in range(1, count):
        pl.when(sp - d >= 0)(lambda: carry_copy(d).wait_send())


def carry_and_total(nz, decays, carried, parts):
    count = 2 * nz
    heads, channels, states = carried.shape
    lanes = 128
    place = lax.axis_index("sp")
    padded = jnp.concatenate([decays, jnp.ones_like(decays)])
    ahead = lax.dynamic_slice_in_dim(padded, place + 1, count - 1, 0)
    coefs = jnp.concatenate([jnp.ones_like(ahead[:1]), jnp.cumprod(ahead[:-1], axis=0)])
    flat = carried.astype(jnp.bfloat16).reshape(-1, lanes)
    rows, width = parts.shape[0] // count, parts.shape[1]
    dma = pltpu.SemaphoreType.DMA
    vmem = functools.partial(pltpu.VMEM, dtype=jnp.bfloat16)
    space = pl.BlockSpec(memory_space=pltpu.VMEM)
    later, total = pl.pallas_call(
        functools.partial(carry_kernel, nz),
        out_shape=(
            jax.ShapeDtypeStruct(flat.shape, jnp.float32),
            jax.ShapeDtypeStruct((rows, width), jnp.float32),
        ),
        in_specs=[pl.BlockSpec(memory_space=pltpu.SMEM), space, space],
        out_specs=(space, space),
        scratch_shapes=[
            vmem((count,) + flat.shape),
            vmem((nz, rows, width)),
            vmem((nz, rows, width)),
            vmem((nz, rows, width)),
            dma((2, count)),
            dma((2, nz)),
            dma((2, nz)),
        ],
        compiler_params=pltpu.CompilerParams(collective_id=2, has_side_effects=True),
        name="carry_and_total",
    )(coefs, flat, parts.astype(jnp.bfloat16))
    return later.reshape(heads, channels, states), total


def dense_grads(normed, cotangent, routes, route_weight, decay_now, gate_mat, up_mat, down_mat):
    sp_count = lax.axis_size("sp")
    experts_count = sp_count // 2
    nz = sp_count // 2
    names = jnp.arange(experts_count, dtype=jnp.int32)[:, None]
    table = jnp.where(routes[None, :, 0] == names, route_weight[None, :, 0], 0.0)
    table = table + jnp.where(routes[None, :, 1] == names, route_weight[None, :, 1], 0.0)
    spread = jnp.broadcast_to(decay_now[:, None], (decay_now.shape[0], table.shape[1]))
    table = jnp.concatenate([table, spread])
    rows_in, cot_all, tables = gather_rows(nz, normed, cotangent, table)
    decays = tables[:, experts_count:, 0]
    weight_all = lax.dynamic_index_in_dim(tables, lax.axis_index("sp") // 2, 1, False).reshape(-1)
    rows_cot = (weight_all[:, None] * cot_all.astype(jnp.float32)).astype(jnp.bfloat16)
    gate_grad, up_grad, down_grad, input_part = expert_grads(
        rows_in, rows_cot, gate_mat, up_mat, down_mat
    )
    normed_grad = total_rows(nz, input_part.astype(jnp.bfloat16)).astype(jnp.float32)
    return gate_grad, up_grad, down_grad, normed_grad, decays


def routed_grads(normed, cotangent, routes, route_weight, gate_mat, up_mat, down_mat):
    sp_count = lax.axis_size("sp")
    tp_count = lax.axis_size("tp")
    tok_rows = normed.shape[0]
    experts_count = sp_count // 2
    capacity = min(tok_rows, 4 * tok_rows // experts_count)
    quarter = D // tp_count
    route_flat = routes.reshape(-1)
    member = (route_flat[:, None] == jnp.arange(experts_count, dtype=jnp.int32)[None, :]).astype(
        jnp.int32
    )
    earlier_count = jnp.sum((jnp.cumsum(member, axis=0) - member) * member, axis=1)
    places = (route_flat * capacity + earlier_count).reshape(tok_rows, 2)
    slot_ids = jnp.arange(experts_count * capacity, dtype=jnp.int32)[:, None]
    first_hit = slot_ids == places[None, :, 0]
    second_hit = slot_ids == places[None, :, 1]
    placing = jnp.logical_or(first_hit, second_hit)
    place_matrix = placing.astype(jnp.bfloat16)
    slot_weight = jnp.sum(
        jnp.where(first_hit, route_weight[None, :, 0], 0.0)
        + jnp.where(second_hit, route_weight[None, :, 1], 0.0),
        axis=1,
    )
    send_in = jnp.dot(place_matrix, normed, preferred_element_type=jnp.float32).astype(jnp.bfloat16)
    send_cot = (
        slot_weight[:, None] * jnp.dot(place_matrix, cotangent, preferred_element_type=jnp.float32)
    ).astype(jnp.bfloat16)
    half_cap = capacity // 2
    part_in, part_cot = (
        lax.all_to_all(
            send_in.reshape(sp_count, half_cap, D), "sp", split_axis=0, concat_axis=0, tiled=True
        ),
        lax.all_to_all(
            send_cot.reshape(sp_count, half_cap, D), "sp", split_axis=0, concat_axis=0, tiled=True
        ),
    )
    other_in, other_cot = swapped((part_in, part_cot), "sp", 0)
    lower_bit = lax.axis_index("sp") % 2 == 0
    recv_in = jnp.concatenate(
        [jnp.where(lower_bit, part_in, other_in), jnp.where(lower_bit, other_in, part_in)], axis=1
    )
    recv_cot = jnp.concatenate(
        [jnp.where(lower_bit, part_cot, other_cot), jnp.where(lower_bit, other_cot, part_cot)],
        axis=1,
    )
    rows_in = recv_in.reshape(-1, D)
    rows_cot = recv_cot.reshape(-1, D)
    gate_grad, up_grad, down_grad, input_part = expert_grads(
        rows_in, rows_cot, gate_mat, up_mat, down_mat
    )
    input_quarter = lax.psum_scatter(input_part, "tp", scatter_dimension=1, tiled=True)
    returned = lax.all_to_all(
        input_quarter.reshape(sp_count, capacity, quarter),
        "sp",
        split_axis=0,
        concat_axis=0,
        tiled=True,
    )
    pair_total = jnp.sum(returned.reshape(experts_count, 2, capacity, quarter), axis=1).reshape(
        -1, quarter
    )
    token_quarter = lax.dot_general(
        placing.astype(jnp.float32), pair_total, (((0,), (0,)), ((), ())), precision=HIGHEST
    )
    normed_grad = lax.all_gather(token_quarter, "tp", axis=1, tiled=True)
    return gate_grad, up_grad, down_grad, normed_grad


def shards(
    tokens,
    norm_gain,
    cotangent,
    routes,
    route_weight,
    gate_weight,
    up_weight,
    down_weight,
    scan_input,
    out_gate,
    step_size,
    decay_rate,
    write_keys,
    read_keys,
    start_state,
    out_proj,
):
    sp_count = lax.axis_size("sp")
    tp_count = lax.axis_size("tp")
    tok_rows = tokens.shape[0]
    experts_count = sp_count // 2
    capacity = min(tok_rows, 4 * tok_rows // experts_count)
    quarter = D // tp_count
    hidden = tokens.astype(jnp.float32)
    inverse = lax.rsqrt(jnp.mean(hidden * hidden, axis=1) + EPS)
    normed = (hidden * inverse[:, None] * norm_gain[None, :]).astype(jnp.bfloat16)
    dense = capacity == tok_rows and tp_count == 4
    mats = (gate_weight[0], up_weight[0], down_weight[0])
    if dense:
        decay_now = jnp.exp(jnp.sum(-decay_rate[:, None] * step_size, axis=1))
        gate_grad, up_grad, down_grad, normed_grad, decays = dense_grads(
            normed, cotangent, routes, route_weight, decay_now, *mats
        )
    else:
        gate_grad, up_grad, down_grad, normed_grad = routed_grads(
            normed, cotangent, routes, route_weight, *mats
        )
    gained = norm_gain[None, :] * normed_grad
    dotted = jnp.sum(hidden * gained, axis=1)
    residual = (
        cotangent.astype(jnp.float32)
        + inverse[:, None] * gained
        - hidden * (inverse**3 * dotted / D)[:, None]
    )
    residual_grad = residual.astype(jnp.bfloat16)
    mix_grad = jnp.dot(residual_grad, out_proj, preferred_element_type=jnp.float32)
    per_group = HEADS // GROUPS
    gated, gate_out_grad, decay_now, carried, state_grad = block_forward(
        scan_input,
        out_gate,
        step_size,
        write_keys,
        read_keys,
        decay_rate,
        start_state[0],
        mix_grad,
        per_group,
    )
    proj_part = lax.dot_general(
        residual_grad, gated, (((0,), (0,)), ((), ())), preferred_element_type=jnp.float32
    )
    if dense:
        later_state, out_proj_grad = carry_and_total(sp_count // 2, decays, carried, proj_part)
    else:
        totals, later_state = prefix(
            (decay_now, carried), "sp", compose, (jnp.ones_like(decay_now), jnp.zeros_like(carried))
        )
        out_proj_grad = lax.psum_scatter(proj_part, "sp", scatter_dimension=0, tiled=True)
    scan_grad, write_grad, read_grad = block_back(
        scan_input,
        step_size,
        write_keys,
        read_keys,
        decay_rate,
        start_state[0],
        state_grad,
        later_state,
        per_group,
    )
    residual_part = lax.dynamic_slice_in_dim(
        residual_grad, lax.axis_index("tp") * quarter, quarter, 1
    )
    return (
        residual_part,
        gate_grad.astype(jnp.bfloat16)[None],
        up_grad.astype(jnp.bfloat16)[None],
        down_grad.astype(jnp.bfloat16)[None],
        out_proj_grad,
        scan_grad,
        gate_out_grad,
        write_grad,
        read_grad,
    )


def solution(mesh):
    return jax.shard_map(
        shards,
        mesh=mesh,
        in_specs=(
            P("sp", None),
            P(),
            P("sp", None),
            P("sp", None),
            P("sp", None),
            P("sp", None, "tp"),
            P("sp", None, "tp"),
            P("sp", "tp", None),
            P("sp", "tp"),
            P("sp", "tp"),
            P("tp", "sp"),
            P("tp"),
            P("sp", "tp"),
            P("sp", "tp"),
            P("sp", "tp", None, None),
            P(None, "tp"),
        ),
        out_specs=(
            P("sp", "tp"),
            P("sp", None, "tp"),
            P("sp", None, "tp"),
            P("sp", "tp", None),
            P("sp", "tp"),
            P("sp", "tp"),
            P("sp", "tp"),
            P("sp", "tp"),
            P("sp", "tp"),
        ),
        check_vma=False,
    )
```
